32 devices in a mesh: grp: 2 (over y), dp: 2 (over x), kv: 4 (over z), tp: 2 (over core).
Axes of the slice: x: 2, y: 2, z: 4, core: 2. Of those that a mesh axis runs over, the one named last changes fastest.
Arguments:
- queries: bfloat16 [4, 1024, 2048], P(('grp', 'dp'), 'kv', 'tp'), parts along dimension 0, may hold values from -10 to 10
- keys: bfloat16 [4, 1024, 512], P(('grp', 'dp'), 'kv', 'tp'), parts along dimension 0, may hold values from -10 to 10
- values: bfloat16 [4, 1024, 512], P(('grp', 'dp'), 'kv', 'tp'), parts along dimension 0, may hold values from -6 to 6
- gate_logits: float32 [4, 2, 1024, 32], P(('grp', 'dp'), None, 'kv', 'tp'), parts along dimension 0, may hold values from -6 to 6
- chosen: int32 [4, 8, 8, 16], P(('grp', 'dp'), 'kv', 'tp'), parts along dimension 0, may hold values from -1 to 15, as said below
- pool_k: float32 [32, 64], replicated, may hold values from 0 to 0.35
- pool_v: float32 [32, 64], replicated, may hold values from 0 to 0.35
- out_gain: float32 [2048], P('tp'), may hold values from 0.1 to 1.9
Outputs:
- attended: bfloat16 [4, 1024, 2048], P(('grp', 'dp'), 'kv', 'tp'), parts along dimension 0
The draws below stay inside these ranges and needn't reach their ends.
There are 2 independent parts, one for each index of `grp`. The reference program is written for one: setup_inputs(seed, part) draws one part's arguments, and reference() takes and returns one part's arrays. A program takes and returns all parts, laid end to end along the dimension named above; an argument that names none is the same for every part. Nothing has to cross between parts.
Inputs may be any that keep to these rules, and one draw needn't show every extreme that they name: Entries are key block numbers (block e holds positions e * 64 to e * 64 + 63) or -1 for none. The list of query block b (positions b * 128 onward) holds the blocks that contain its own positions, other distinct blocks that begin before it, and -1 in its remaining entries. For the query blocks of one span of 256 positions and one key head, the blocks chosen from any other span number at most 2; in every draw some span reaches 2.
All inputs are finite; a program needn't handle non-finite values.
Results may differ from the reference program's by a relative error of at most 0.0079.
Values may be sent and summed in bfloat16 or wider, within the bound.
A program may use at most 64 MiB of HBM per device.

```python
import jax
import jax.numpy as jnp
from jax import lax

H = 32
G = 8
DH = 64
HPG = 4
CMP_STRIDE = 16
CMP_BLOCK = 32
SLC = 64
QB = 128
NSEL = 16
MOST = 2
TOK_DEV = 256
SEQS = 2
SEQLEN = 1024
N_KV = 4


def base_field(key, shape):
    return jnp.clip(jax.random.normal(key, shape, jnp.float32), -6.0, 6.0)


def draw_queries(key, part):
    field = base_field(jax.random.fold_in(key, 1), (SEQS, SEQLEN, H * DH))
    return field.astype(jnp.bfloat16)


def draw_keys(key, part):
    field = base_field(jax.random.fold_in(key, 2), (SEQS, SEQLEN, G * DH))
    return field.astype(jnp.bfloat16)


def draw_chosen(key, part):
    nqb = SEQLEN // QB
    per_owner = TOK_DEV // SLC
    total = SEQLEN // SLC
    own = QB // SLC
    per_span = TOK_DEV // QB
    base = jax.random.fold_in(key, 101)
    pop_key, set_key, pick_key = jax.random.split(base, 3)
    favour = jax.random.randint(pop_key, (SEQS, total), 0, 3)
    raw = jax.random.randint(set_key, (SEQS, N_KV, G, N_KV, per_owner), 0, 65536)
    setscore = (raw - favour.reshape(SEQS, 1, 1, N_KV, per_owner) * 40000) * per_owner + jnp.arange(per_owner)
    rank = jnp.sum(setscore[..., None, :] < setscore[..., :, None], axis=-1)
    inset = rank < MOST
    blocks = jnp.arange(nqb)
    span = blocks // per_span
    inset_q = inset[:, span].reshape(SEQS, nqb, G, total)
    number = jnp.arange(total)
    owner = number // per_owner
    remote = owner[None, :] < span[:, None]
    earlier = (owner[None, :] == span[:, None]) & (number[None, :] < blocks[:, None] * own)
    mine = number[None, :] // own == blocks[:, None]
    near = (owner[None, :] == span[:, None] - 1) | (owner[None, :] == span[:, None] - N_KV // 2) & (span[:, None] >= N_KV // 2)
    avail = remote[None, :, None, :] & inset_q | earlier[None, :, None, :]
    forced = mine[None, :, None, :] | (remote & near)[None, :, None, :] & inset_q
    noise = jax.random.randint(pick_key, (SEQS, nqb, G, total), 0, 65536) - favour[:, None, None, :] * 20000
    prio = jnp.where(forced, 0, jnp.where(avail, noise + 40001, 1 << 22))
    order = jnp.argsort(prio * total + number, axis=-1)[..., :NSEL]
    picked = jnp.take_along_axis(prio, order, axis=-1)
    return jnp.where(picked < 1 << 22, order, -1).astype(jnp.int32)


def levels(stream_key, dims, shards, smallest, largest):
    gain = 1.0
    for position, blocks in shards:
        draws = jax.random.uniform(jax.random.fold_in(jax.random.fold_in(stream_key, 6), position), (blocks,), jnp.float32, smallest / len(shards), largest / len(shards))
        gain = gain * jnp.repeat(jnp.exp(draws), dims[position] // blocks).reshape((-1,) + (1,) * (len(dims) - 1 - position))
    return gain


def normal_values(own_key, shape, deviation, most, cuts=(), held_as=jnp.bfloat16):
    result = deviation * jax.random.normal(own_key, shape, jnp.float32)
    if cuts:
        result = result * levels(own_key, shape, cuts, -0.22, 0.18)
    return jnp.clip(result, -most, most).astype(held_as)


def setup_inputs(seed: int = 0, part: int = 0) -> dict:
    streams_of = jax.random.split(jax.random.key(seed), 9)
    own_keys = jax.random.split(jax.random.fold_in(streams_of[8], part), 9)
    return {
        "queries": draw_queries(jax.random.fold_in(jax.random.fold_in(streams_of[8], part), 71), part),
        "keys": draw_keys(jax.random.fold_in(jax.random.fold_in(streams_of[8], part), 71), part),
        "values": normal_values(own_keys[2], (SEQS, SEQLEN, G * DH), 1.0, 6.0, ((0, 2), (1, 4), (2, 2))),
        "gate_logits": normal_values(own_keys[3], (SEQS, 2, SEQLEN, H), 1.5, 6.0, ((0, 2), (2, 4), (3, 2)), jnp.float32),
        "chosen": draw_chosen(jax.random.fold_in(jax.random.fold_in(streams_of[8], part), 71), part),
        "pool_k": jnp.clip(jax.random.uniform(streams_of[5], (CMP_BLOCK, DH), jnp.float32, 0.0, 0.35), 0.0, 0.35),
        "pool_v": jnp.clip(jax.random.uniform(streams_of[6], (CMP_BLOCK, DH), jnp.float32, 0.0, 0.35), 0.0, 0.35),
        "out_gain": jnp.clip(1.0 + 0.18 * jax.random.normal(streams_of[7], (H * DH,), jnp.float32), 0.1, 1.9),
    }


THETA = 500000.0
EPS = 1e-06
NEG = -1e+30

def rotate(matrix, start, heads):
    length = matrix.shape[0]
    half = DH // 2
    place = (start + jnp.arange(length)).astype(jnp.float32)
    freq = jnp.power(jnp.float32(THETA), -(2.0 * jnp.arange(half).astype(jnp.float32)) / DH)
    angle = place[:, None] * freq[None, :]
    cosine = jnp.cos(angle)[:, None, :]
    sine = jnp.sin(angle)[:, None, :]
    parts = matrix.reshape(length, heads, DH).astype(jnp.float32)
    first = parts[..., :half]
    second = parts[..., half:]
    turned = jnp.concatenate([first * cosine - second * sine, second * cosine + first * sine], -1)
    return turned.reshape(length, heads * DH).astype(jnp.bfloat16)

def compress(extended, pool, groups):
    count = extended.shape[0] // CMP_STRIDE - 1
    parts = extended.reshape(count + 1, CMP_STRIDE, groups, DH).astype(jnp.float32)
    lower = jnp.einsum('nigd,id->ngd', parts[:-1], pool[:CMP_STRIDE], precision=lax.Precision.HIGHEST)
    upper = jnp.einsum('nigd,id->ngd', parts[1:], pool[CMP_STRIDE:], precision=lax.Precision.HIGHEST)
    return (lower + upper).astype(jnp.bfloat16)

def reference(queries, keys, values, gate_logits, chosen, pool_k, pool_v, out_gain):
    scale = DH ** (-0.5)

    def one_sequence(item):
        query_seq, key_seq, value_seq, logits, lists = item
        length = query_seq.shape[0]
        query_turned = rotate(query_seq, 0, H)
        key_turned = rotate(key_seq, 0, G)
        padding = jnp.zeros((CMP_STRIDE, G * DH), key_seq.dtype)
        key_summary = compress(jnp.concatenate([key_seq, padding], 0), pool_k, G).astype(jnp.float32)
        value_summary = compress(jnp.concatenate([value_seq, padding], 0), pool_v, G).astype(jnp.float32)
        count = length // CMP_STRIDE
        ends = jnp.arange(count) * CMP_STRIDE + CMP_BLOCK - 1
        key_blocks = key_turned.reshape(length // SLC, SLC, G, DH)
        value_blocks = value_seq.reshape(length // SLC, SLC, G, DH)
        group_pick = jnp.arange(G)[:, None]

        def block(index):
            start = index * QB
            place = start + jnp.arange(QB)
            query_rows = lax.dynamic_slice_in_dim(query_seq, start, QB, 0).reshape(QB, G, HPG, DH).astype(jnp.float32)
            query_turn = lax.dynamic_slice_in_dim(query_turned, start, QB, 0).reshape(QB, G, HPG, DH).astype(jnp.float32)
            score = jnp.einsum('tghd,ngd->ghtn', query_rows, key_summary) * scale
            allow = (ends[None, :] <= place[:, None])[None, None]
            score = jnp.where(allow, score, NEG)
            top = lax.optimization_barrier(jnp.max(score, -1, keepdims=True))
            weight = jnp.where(allow, jnp.exp(score - top), 0.0)
            total = jnp.maximum(lax.optimization_barrier(jnp.sum(weight, -1)), 1.0)
            rounded = lax.optimization_barrier(weight.astype(jnp.bfloat16)).astype(jnp.float32)
            summary_out = jnp.einsum('ghtn,ngd->ghtd', rounded, value_summary) / total[..., None]
            picks = lists[index]
            safe = jnp.maximum(picks, 0)
            key_sel = key_blocks[safe, :, group_pick, :].astype(jnp.float32)
            value_sel = value_blocks[safe, :, group_pick, :].reshape(G, NSEL * SLC, DH).astype(jnp.float32)
            key_place = (safe[..., None] * SLC + jnp.arange(SLC)).reshape(G, NSEL * SLC)
            live = jnp.broadcast_to(picks[..., None] >= 0, (G, NSEL, SLC)).reshape(G, NSEL * SLC)
            allow_sel = (live[:, None, :] & (key_place[:, None, :] <= place[None, :, None]))[:, None]
            chosen_score = jnp.einsum('tghd,gnkd->ghtnk', query_turn, key_sel).reshape(G, HPG, QB, NSEL * SLC) * scale
            chosen_score = jnp.where(allow_sel, chosen_score, NEG)
            top_sel = lax.optimization_barrier(jnp.max(chosen_score, -1, keepdims=True))
            weight_sel = jnp.where(allow_sel, jnp.exp(chosen_score - top_sel), 0.0)
            total_sel = lax.optimization_barrier(jnp.sum(weight_sel, -1))
            rounded_sel = lax.optimization_barrier(weight_sel.astype(jnp.bfloat16)).astype(jnp.float32)
            chosen_out = jnp.einsum('ghtk,gkd->ghtd', rounded_sel, value_sel) / total_sel[..., None]
            gates = jax.nn.sigmoid(lax.dynamic_slice_in_dim(logits, start, QB, 1))
            gates = gates.reshape(2, QB, G, HPG).transpose(0, 2, 3, 1)
            mixed = gates[0][..., None] * summary_out + gates[1][..., None] * chosen_out
            mixed = mixed.transpose(2, 0, 1, 3).reshape(QB, H, DH)
            normed = mixed * lax.rsqrt(lax.optimization_barrier(jnp.mean(mixed * mixed, -1, keepdims=True)) + EPS) * out_gain.reshape(H, DH)
            return normed.reshape(QB, H * DH).astype(jnp.bfloat16)
        return lax.map(block, jnp.arange(length // QB)).reshape(length, H * DH)
    return lax.map(one_sequence, (queries, keys, values, gate_logits, chosen))
```

```python
import functools

import jax
import jax.numpy as jnp
import numpy as np
from jax import lax
from jax.experimental import pallas as pl
from jax.experimental.pallas import tpu as pltpu
from jax.sharding import PartitionSpec as P

DH = 64
CMP_STRIDE = 16
CMP_BLOCK = 32
SLC = 64
QB = 128
MOST = 2
THETA = 500000.0
EPS = 1e-06
NEG = -1e30
LOG2E = 1.4426950408889634
WIDE = 2 * DH
ONES = 16
MESH = pl.DeviceIdType.MESH


def rope_constants(n, length):
    half = DH // 2
    freq = THETA ** (-2.0 * (np.arange(WIDE) % half) / DH)
    within = np.arange(length)[:, None] * freq[None, :]
    start = np.arange(n)[:, None] * length * freq[None, :]
    base = np.stack([np.cos(within), np.sin(within)]).astype(np.float32)
    shift = np.stack([np.cos(start), np.sin(start)], 1).astype(np.float32)
    return base, shift


def kernel(
    n, q_hbm, k_hbm, v_hbm, gate_hbm, list_hbm, pk_hbm, pv_hbm, gain_hbm, base_hbm, shift_hbm,
    out_ref,
    q_ref, kv_ref, gate_ref, list_ref, pool_ref, gain_ref, base_ref, shift_ref,
    near, qt, kk, kkr, vt, vtr, sall, skk, svt, flag, own_bias, far_bias, tri, spread_map,
    req, reqbuf, sendk, sendv, recvk, recvv, wslot, slot_top,
    top, total, acc, stot, sacc,
    local, near_send, near_recv, req_send, req_recv, k_send, k_recv, v_send, v_recv,
    sum_send, sum_recv,
):
    me = lax.axis_index("kv")
    length = q_ref.shape[0]
    heads = q_ref.shape[1] // DH
    width = kv_ref.shape[2]
    groups = width // DH
    per_group = heads // groups
    pairs = per_group // 2
    slabs = groups // 2
    qblocks = length // QB
    per = length // SLC
    count = length // CMP_STRIDE
    size = MOST * SLC
    scale = DH ** (-0.5) * LOG2E
    f32, bf16 = jnp.float32, jnp.bfloat16

    barrier = pltpu.get_barrier_semaphore()

    @pl.when(me >= 1)
    def _():
        pl.semaphore_signal(barrier, inc=1, device_id={"kv": me - 1}, device_id_type=MESH)

        @pl.loop(me + 1, n)
        def _(r):
            pl.semaphore_signal(barrier, inc=1, device_id={"kv": r}, device_id_type=MESH)

    fetches = [
        pltpu.make_async_copy(src, dst, local.at[i])
        for i, (src, dst) in enumerate(
            (
                (k_hbm.at[0], kv_ref.at[0]),
                (v_hbm.at[0], kv_ref.at[1]),
                (list_hbm.at[0], list_ref),
                (base_hbm, base_ref),
                (shift_hbm, shift_ref),
                (q_hbm.at[0], q_ref),
                (pk_hbm, pool_ref.at[0]),
                (pv_hbm, pool_ref.at[1]),
                (gate_hbm.at[0], gate_ref),
                (gain_hbm, gain_ref),
            )
        )
    ]
    for fetch in fetches:
        fetch.start()

    def remote(src, dst, send, recv, peer):
        return pltpu.make_async_remote_copy(
            src_ref=src, dst_ref=dst, send_sem=send, recv_sem=recv,
            device_id={"kv": peer}, device_id_type=MESH,
        )

    def give_near(w, peer):
        return remote(kv_ref.at[w], near.at[w], near_send.at[w], near_recv.at[w], peer)

    def ask(s, origin):
        return remote(req.at[s], reqbuf.at[origin], req_send.at[s], req_recv.at[origin], s + 1)

    def give_k(r, s):
        return remote(sendk.at[r], recvk.at[s], k_send.at[r], k_recv.at[s], r)

    def give_v(r, s):
        return remote(sendv.at[r], recvv.at[s], v_send.at[r], v_recv.at[s], r)

    def give_sum(r, s):
        return remote(sall.at[s], sall.at[s], sum_send.at[r], sum_recv.at[s], r)

    def iota(shape, axis):
        return lax.broadcasted_iota(jnp.int32, shape, axis)

    fetches[0].wait()
    fetches[1].wait()
    pl.semaphore_wait(barrier, jnp.where(me < n - 1, 1, 0) + jnp.maximum(me - 1, 0))

    @pl.when(me < n - 1)
    def _():
        give_near(0, me + 1).start()
        give_near(1, me + 1).start()

    lanes = flag.shape[1]
    rows = qblocks * groups

    def column(x, at):
        spot = iota(x.shape, 1) == at
        picked = jnp.sum(jnp.where(spot, x.astype(f32), 0.0), 1, keepdims=True)
        return jnp.broadcast_to(picked, (x.shape[0], QB))

    fetches[2].wait()
    lists = jnp.concatenate([list_ref[b] for b in range(qblocks)], 0)
    lane = iota((rows, lanes), 1)
    member = jnp.zeros((rows, lanes), jnp.int32)
    for i in range(lists.shape[1]):
        member = jnp.where(lists[:, i : i + 1] == lane, 1, member)
    union = member[:groups]
    for b in range(1, qblocks):
        union = jnp.maximum(union, member[b * groups : (b + 1) * groups])
    union = jnp.concatenate([union] * qblocks, 0)
    inner = lane % per
    rank = jnp.zeros_like(union)
    for d in range(1, per):
        rank = rank + jnp.where(inner >= d, pltpu.roll(union, d, 1), 0)

    def first_of(x):
        found = x
        for d in range(1, per):
            found = found + pltpu.roll(x, lanes - d, 1)
        return found

    asked = []
    for j in range(MOST):
        hit = (union == 1) & (rank == j)
        asked.append(first_of(jnp.where(hit, inner, 0))[:groups])
        flag[j * rows : (j + 1) * rows, :] = first_of(jnp.where(hit, member, 0))
    asked = jnp.concatenate(asked, 0)
    low_row = iota((1, WIDE), 1) < DH

    @pl.loop(0, me)
    def _(s):
        ids = column(asked, s * per)
        for j in range(MOST):
            for p in range(slabs):
                at = j * groups + 2 * p
                req[s, j * slabs + p : j * slabs + p + 1, :] = jnp.where(
                    low_row, ids[at : at + 1], ids[at + 1 : at + 2]
                )

    @pl.loop(0, me - 1)
    def _(s):
        ask(s, me).start()

    for i in range(per):
        own_bias[i] = jnp.where(column(member, me * per + i) > 0.5, 0.0, NEG)
    tri[...] = jnp.where(iota((QB, QB), 0) <= iota((QB, QB), 1), 0.0, NEG)

    def lane_map(shape, source):
        return jnp.where(iota(shape, 0) == source(iota(shape, 1)), 1.0, 0.0).astype(bf16)

    half = DH // 2
    partner_map = lane_map((width, width), lambda c: c - c % DH + (c + half) % DH)
    wide_shape = (width, groups * WIDE)
    spread_map[...] = lane_map(wide_shape, lambda c: c // WIDE * DH + c % DH)
    spread_partner = lane_map(wide_shape, lambda c: c // WIDE * DH + (c + half) % DH)
    eye = lane_map((width, width), lambda c: c)

    def mapped(x, lanes_to):
        return jnp.dot(x, lanes_to, preferred_element_type=f32)

    def score(keys, queries):
        return lax.dot_general(
            keys, queries, (((1,), (1,)), ((), ())), preferred_element_type=f32
        )

    fetches[3].wait()
    fetches[4].wait()
    sign = jnp.where(iota((1, WIDE), 1) % DH < half, -1.0, 1.0)

    def tables(span):
        cos_in, sin_in = base_ref[0], base_ref[1]
        cos_at, sin_at = shift_ref[span, 0:1], shift_ref[span, 1:2]
        cosine = cos_in * cos_at - sin_in * sin_at
        sine = (sin_in * cos_at + cos_in * sin_at) * sign
        return cosine, sine

    low = iota((length, WIDE), 1) < DH
    cosine, sine = tables(me)
    plain = mapped(kv_ref[0], spread_map[...])
    other = mapped(kv_ref[0], spread_partner)
    for g in range(groups):
        cols = slice(g * WIDE, (g + 1) * WIDE)
        turned = plain[:, cols] * cosine + other[:, cols] * sine
        kk[g, 0] = jnp.where(low, turned, 0.0).astype(bf16)
        kk[g, 1] = jnp.where(low, 0.0, turned).astype(bf16)

    def flipped(x):
        return score(eye, x).astype(bf16)

    flip = flipped(kv_ref[1])
    for g in range(groups):
        vt[g, :DH] = flip[g * DH : (g + 1) * DH]
        vt[g, DH:] = jnp.ones((ONES, length), bf16)
        vtr[g, DH:] = jnp.ones((ONES, size), bf16)
        svt[g, DH:] = jnp.ones((ONES, n * count), bf16)

    cosine = cosine * scale
    sine = sine * scale
    fetches[5].wait()
    span_slabs = width // WIDE
    for p in range(heads // 2 // span_slabs):
        x = q_ref[:, p * width : (p + 1) * width]
        other = mapped(x, partner_map)
        for i in range(span_slabs):
            cols = slice(i * WIDE, (i + 1) * WIDE)
            qt[p * span_slabs + i] = (x[:, cols].astype(f32) * cosine + other[:, cols] * sine).astype(
                bf16
            )

    @pl.loop(0, groups, unroll=2)
    def _(g):
        both = kk[g].reshape(2 * length, WIDE)
        values = vt[g]
        for pair in range(pairs):
            raw = score(both, qt[g * pairs + pair])
            for e in range(2):
                h = g * per_group + 2 * pair + e
                weights, tops = [], []
                for b in range(qblocks):
                    cols = slice(b * QB, (b + 1) * QB)
                    parts = []
                    for i in range((b + 1) * QB // SLC):
                        x = raw[e * length + i * SLC : e * length + (i + 1) * SLC, cols]
                        if i * SLC < b * QB:
                            x = x + own_bias[i, pl.ds(b * groups + g, 1), :]
                        else:
                            x = x + tri[i * SLC - b * QB : (i + 1) * SLC - b * QB, :]
                        parts.append(x)
                    x = jnp.concatenate(parts, 0)
                    peak = jnp.max(x, 0, keepdims=True)
                    w = jnp.exp2(x - peak).astype(bf16)
                    if x.shape[0] < length:
                        w = jnp.concatenate([w, jnp.zeros((length - x.shape[0], QB), bf16)], 0)
                    weights.append(w)
                    tops.append(peak)
                found = jnp.dot(
                    values, jnp.concatenate(weights, 1), preferred_element_type=f32
                )
                top[h] = jnp.concatenate(tops, 1)
                total[h] = found[DH : DH + 1]
                acc[h] = found[:DH]

    fetches[6].wait()
    fetches[7].wait()

    def summarize(w, x, following, p):
        pool = pool_ref[w]
        pool = jnp.concatenate([pool, pool], 1)
        cols = slice(p * WIDE, (p + 1) * WIDE)
        x = x[:, cols].astype(f32)
        after = jnp.concatenate([x[CMP_STRIDE:], following[:, cols].astype(f32)], 0)
        shape = (count, CMP_STRIDE, WIDE)
        z = x.reshape(shape) * pool[None, :CMP_STRIDE] + after.reshape(shape) * pool[None, CMP_STRIDE:]
        found = jnp.sum(z, 1)
        return (found * scale if w == 0 else found).astype(bf16)

    for w in range(2):
        for p in range(slabs):
            sall[me, w, :, p * WIDE : (p + 1) * WIDE] = summarize(
                w, kv_ref[w], jnp.zeros((CMP_STRIDE, width), bf16), p
            )

    def gather(source, w_rows, dst, at):
        for j in range(MOST):
            for p in range(slabs):
                cols = slice(p * WIDE, (p + 1) * WIDE)
                pick = w_rows[j * slabs + p : j * slabs + p + 1, :]
                block = None
                for i in range(per):
                    weight = jnp.broadcast_to(jnp.where(pick == i, 1.0, 0.0), (SLC, WIDE))
                    term = source[i * SLC : (i + 1) * SLC, cols] * weight.astype(bf16)
                    block = term if block is None else block + term
                dst[at, j * SLC : (j + 1) * SLC, cols] = block

    @pl.when(me >= 1)
    def _():
        s = me - 1
        give_near(0, me).wait_recv()
        cosine, sine = tables(s)
        x = near[0]
        other = mapped(x, partner_map)
        slab = []
        for p in range(slabs):
            cols = slice(p * WIDE, (p + 1) * WIDE)
            slab.append((x[:, cols].astype(f32) * cosine + other[:, cols] * sine).astype(bf16))
        turned = jnp.concatenate(slab, 1)

        @pl.loop(0, n - 1 - me)
        def _(d):
            r = n - 1 - d
            ask(s, r).wait_recv()
            gather(turned, reqbuf[r], sendk, r)
            give_k(r, s).start()

        gather(turned, req[s], recvk, s)
        give_near(1, me).wait_recv()
        for w in range(2):
            for p in range(slabs):
                sall[s, w, :, p * WIDE : (p + 1) * WIDE] = summarize(
                    w, near[w], kv_ref[w, :CMP_STRIDE], p
                )

        @pl.loop(0, n - 1 - me)
        def _(d):
            r = n - 1 - d
            give_sum(r, s).start()
            gather(near[1], reqbuf[r], sendv, r)
            give_v(r, s).start()

        gather(near[1], req[s], recvv, s)

    low_size = iota((size, WIDE), 1) < DH

    def slot_scores(s):
        far_bias[...] = jnp.where(column(flag[...], s * per) > 0.5, 0.0, NEG)
        wide = mapped(recvk[s], spread_map[...])
        for g in range(groups):
            x = wide[:, g * WIDE : (g + 1) * WIDE]
            kkr[g, 0] = jnp.where(low_size, x, 0.0).astype(bf16)
            kkr[g, 1] = jnp.where(low_size, 0.0, x).astype(bf16)

        @pl.loop(0, groups, unroll=2)
        def _(g):
            rowed = [
                jnp.concatenate(
                    [
                        far_bias[pl.ds((j * qblocks + b) * groups + g, 1), :]
                        for b in range(qblocks)
                    ],
                    1,
                )
                for j in range(MOST)
            ]
            both = kkr[g].reshape(2 * size, WIDE)
            for pair in range(pairs):
                raw = score(both, qt[g * pairs + pair])
                for e in range(2):
                    h = g * per_group + 2 * pair + e
                    x = jnp.concatenate(
                        [
                            raw[e * size + j * SLC : e * size + (j + 1) * SLC] + rowed[j]
                            for j in range(MOST)
                        ],
                        0,
                    )
                    peak = jnp.max(x, 0, keepdims=True)
                    slot_top[s, h] = peak
                    wslot[s, h] = jnp.exp2(x - peak).astype(bf16)

    def slot_values(s):
        flip = flipped(recvv[s])
        for g in range(groups):
            vtr[g, :DH] = flip[g * DH : (g + 1) * DH]

        @pl.loop(0, groups, unroll=2)
        def _(g):
            values = vtr[g]
            for o in range(per_group):
                h = g * per_group + o
                found = jnp.dot(values, wslot[s, h], preferred_element_type=f32)
                old, fresh = top[h], slot_top[s, h]
                peak = jnp.maximum(old, fresh)
                keep, gain = jnp.exp2(old - peak), jnp.exp2(fresh - peak)
                top[h] = peak
                total[h] = total[h] * keep + found[DH : DH + 1] * gain
                acc[h] = acc[h] * keep + found[:DH] * gain

    @pl.when(me >= 1)
    def _():
        slot_scores(me - 1)
        slot_values(me - 1)

    @pl.loop(0, me - 1)
    def _(s):
        give_k(me, s).wait_recv()
        slot_scores(s)

    @pl.loop(0, me - 1)
    def _(s):
        give_sum(me, s).wait_recv()

    blocks = n * count
    known = iota((blocks, width), 0) < (me + 1) * count
    sum_k = jnp.where(known, sall[:, 0].reshape(blocks, width).astype(f32), 0.0).astype(bf16)
    sum_v = jnp.where(known, sall[:, 1].reshape(blocks, width).astype(f32), 0.0).astype(bf16)
    wide = mapped(sum_k, spread_map[...])
    low_blocks = iota((blocks, WIDE), 1) < DH
    flip = flipped(sum_v)
    for g in range(groups):
        x = wide[:, g * WIDE : (g + 1) * WIDE]
        skk[g, 0] = jnp.where(low_blocks, x, 0.0).astype(bf16)
        skk[g, 1] = jnp.where(low_blocks, 0.0, x).astype(bf16)
        svt[g, :DH] = flip[g * DH : (g + 1) * DH]
    part_at = iota((blocks, length), 0)
    time_at = iota((blocks, length), 1) + me * length
    sbias = jnp.where(part_at * CMP_STRIDE + CMP_BLOCK - 1 <= time_at, 0.0, NEG)
    for g in range(groups):
        both = skk[g].reshape(2 * blocks, WIDE)
        for pair in range(pairs):
            at = g * pairs + pair
            raw = score(both, q_ref[:, at * WIDE : (at + 1) * WIDE])
            for e in range(2):
                x = raw[e * blocks : (e + 1) * blocks] + sbias
                peak = jnp.maximum(jnp.max(x, 0, keepdims=True), 0.1 * NEG)
                w = jnp.exp2(x - peak).astype(bf16)
                found = jnp.dot(svt[g], w, preferred_element_type=f32)
                h = g * per_group + 2 * pair + e
                stot[h] = found[DH : DH + 1]
                sacc[h] = found[:DH]

    @pl.loop(0, me - 1)
    def _(s):
        give_v(me, s).wait_recv()
        slot_values(s)

    fetches[8].wait()
    fetches[9].wait()
    for pair in range(heads // 2):
        both = []
        for e in range(2):
            h = 2 * pair + e
            first, second = (
                1.0 / (1.0 + jnp.exp(-gate_ref[w, h : h + 1])) for w in range(2)
            )
            mixed = sacc[h] * (first / jnp.maximum(stot[h], 1.0)) + acc[h] * (
                second / total[h]
            )
            mean = jnp.sum(mixed * mixed, 0, keepdims=True) * (1.0 / DH)
            both.append(mixed * lax.rsqrt(mean + EPS))
        cols = slice(pair * WIDE, (pair + 1) * WIDE)
        flat = jnp.concatenate(both, 0).T
        out_ref[0, :, cols] = (flat * gain_ref[:, cols]).astype(bf16)

    @pl.when(me < n - 1)
    def _():
        give_near(0, me + 1).wait_send()
        give_near(1, me + 1).wait_send()

    @pl.loop(0, me - 1)
    def _(s):
        ask(s, me).wait_send()

    @pl.when(me >= 1)
    def _():
        @pl.loop(me + 1, n)
        def _(r):
            give_k(r, me - 1).wait_send()
            give_v(r, me - 1).wait_send()
            give_sum(r, me - 1).wait_send()


def per_device(queries, keys, values, gate_logits, chosen, pool_k, pool_v, out_gain):
    n = lax.axis_size("kv")
    length = queries.shape[1]
    groups = keys.shape[2] // DH
    heads = queries.shape[2] // DH
    qblocks = length // QB
    per = length // SLC
    count = length // CMP_STRIDE
    lanes = -(-n * per // 128) * 128
    rows = qblocks * groups
    width = groups * DH
    size = MOST * SLC
    slabs = groups // 2
    asked = -(-MOST * slabs // 8) * 8
    gates = gate_logits.transpose(0, 1, 3, 2)
    base, shift = rope_constants(n, length)
    bf16, f32, i32 = jnp.bfloat16, jnp.float32, jnp.int32
    vm, dma = pltpu.VMEM, pltpu.SemaphoreType.DMA
    scratch = [
        vm((length, heads * DH), bf16),
        vm((2, length, width), bf16),
        vm((2, heads, length), f32),
        vm(chosen.shape[1:], i32),
        vm((2, CMP_BLOCK, DH), f32),
        vm((1, heads * DH), f32),
        vm(base.shape, f32),
        vm(shift.shape, f32),
        vm((2, length, width), bf16),
        vm((heads // 2, length, WIDE), bf16),
        vm((groups, 2, length, WIDE), bf16),
        vm((groups, 2, size, WIDE), bf16),
        vm((groups, DH + ONES, length), bf16),
        vm((groups, DH + ONES, size), bf16),
        vm((n, 2, count, width), bf16),
        vm((groups, 2, n * count, WIDE), bf16),
        vm((groups, DH + ONES, n * count), bf16),
        vm((MOST * rows, lanes), i32),
        vm((per, rows, QB), f32),
        vm((MOST * rows, QB), f32),
        vm((QB, QB), f32),
        vm((width, groups * WIDE), bf16),
        vm((n, asked, WIDE), f32),
        vm((n, asked, WIDE), f32),
        vm((n, size, width), bf16),
        vm((n, size, width), bf16),
        vm((n, size, width), bf16),
        vm((n, size, width), bf16),
        vm((n, heads, size, length), bf16),
        vm((n, heads, 1, length), f32),
        vm((heads, 1, length), f32),
        vm((heads, 1, length), f32),
        vm((heads, DH, length), f32),
        vm((heads, 1, length), f32),
        vm((heads, DH, length), f32),
        dma((10,)), dma((2,)), dma((2,)),
        dma((n,)), dma((n,)), dma((n,)), dma((n,)), dma((n,)), dma((n,)), dma((n,)), dma((n,)),
    ]
    operands = (queries, keys, values, gates, chosen, pool_k, pool_v, out_gain[None], base, shift)
    return pl.pallas_call(
        functools.partial(kernel, n),
        out_shape=jax.ShapeDtypeStruct(queries.shape, bf16),
        in_specs=[pl.BlockSpec(memory_space=pltpu.HBM)] * 10,
        out_specs=pl.BlockSpec(memory_space=pltpu.VMEM),
        scratch_shapes=scratch,
        compiler_params=pltpu.CompilerParams(
            collective_id=0, has_side_effects=True, vmem_limit_bytes=44 << 20
        ),
    )(*(pltpu.with_memory_space_constraint(x, pltpu.HBM) for x in operands))


def solution(mesh):
    in_specs = (
        P(("grp", "dp"), "kv", "tp"),
        P(("grp", "dp"), "kv", "tp"),
        P(("grp", "dp"), "kv", "tp"),
        P(("grp", "dp"), None, "kv", "tp"),
        P(("grp", "dp"), "kv", "tp", None),
        P(),
        P(),
        P("tp"),
    )
    out_specs = P(("grp", "dp"), "kv", "tp")
    return jax.shard_map(
        per_device, mesh=mesh, in_specs=in_specs, out_specs=out_specs, check_vma=False
    )
```

```python
import functools

import jax
import jax.numpy as jnp
import numpy as np
from jax import lax
from jax.experimental import pallas as pl
from jax.experimental.pallas import tpu as pltpu
from jax.sharding import PartitionSpec as P

DH = 64
CMP_STRIDE = 16
CMP_BLOCK = 32
SLC = 64
QB = 128
MOST = 2
THETA = 500000.0
EPS = 1e-06
NEG = -1e30
LOG2E = 1.4426950408889634
WIDE = 2 * DH
ONES = 16
MESH = pl.DeviceIdType.MESH


def rope_constants(n, length):
    half = DH // 2
    freq = THETA ** (-2.0 * (np.arange(WIDE) % half) / DH)
    within = np.arange(length)[:, None] * freq[None, :]
    start = np.arange(n)[:, None] * length * freq[None, :]
    base = np.stack([np.cos(within), np.sin(within)]).astype(np.float32)
    shift = np.stack([np.cos(start), np.sin(start)], 1).astype(np.float32)
    return base, shift


def kernel(
    n, q_hbm, k_hbm, v_hbm, gate_hbm, list_hbm, pk_hbm, pv_hbm, gain_hbm, base_hbm, shift_hbm,
    out_ref,
    q_ref, kv_ref, gate_ref, list_ref, pool_ref, gain_ref, base_ref, shift_ref,
    near, qraw, qt, kt, vt, sall, sks, svt, wsum, flag, own_bias, far_bias, tri,
    req, reqbuf, reqlast, edge, lastsum, sendk, sendv, recvk, recvv, wslot, slot_top,
    top, total, acc, stot, sacc,
    local, near_send, near_recv, req_send, req_recv, k_send, k_recv, v_send, v_recv,
    sum_send, sum_recv, last_send, last_recv,
):
    me = lax.axis_index("kv")
    length = q_ref.shape[0]
    heads = q_ref.shape[1] // DH
    width = kv_ref.shape[2]
    groups = width // DH
    per_group = heads // groups
    pairs = per_group // 2
    slabs = groups // 2
    qblocks = length // QB
    per = length // SLC
    count = length // CMP_STRIDE
    size = MOST * SLC
    scale = DH ** (-0.5) * LOG2E
    f32, bf16 = jnp.float32, jnp.bfloat16

    barrier = pltpu.get_barrier_semaphore()

    @pl.when(me >= 1)
    def _():
        pl.semaphore_signal(barrier, inc=1, device_id={"kv": me - 1}, device_id_type=MESH)

        @pl.loop(me + 1, n)
        def _(r):
            pl.semaphore_signal(barrier, inc=1, device_id={"kv": r}, device_id_type=MESH)

    fetches = [
        pltpu.make_async_copy(src, dst, local.at[i])
        for i, (src, dst) in enumerate(
            (
                (k_hbm.at[0], kv_ref.at[0]),
                (v_hbm.at[0], kv_ref.at[1]),
                (list_hbm.at[0], list_ref),
                (base_hbm, base_ref),
                (shift_hbm, shift_ref),
                (q_hbm.at[0], q_ref),
                (pk_hbm, pool_ref.at[0]),
                (pv_hbm, pool_ref.at[1]),
                (gate_hbm.at[0], gate_ref),
                (gain_hbm, gain_ref),
            )
        )
    ]
    for fetch in fetches:
        fetch.start()

    def remote(src, dst, send, recv, peer):
        return pltpu.make_async_remote_copy(
            src_ref=src, dst_ref=dst, send_sem=send, recv_sem=recv,
            device_id={"kv": peer}, device_id_type=MESH,
        )

    def give_near(w, peer):
        return remote(kv_ref.at[w], near.at[w], near_send.at[w], near_recv.at[w], peer)

    def ask(s, origin):
        return remote(req.at[s], reqbuf.at[origin], req_send.at[s], req_recv.at[origin], s + 1)

    def give_k(r, s):
        return remote(sendk.at[r], recvk.at[s], k_send.at[r], k_recv.at[s], r)

    def give_v(r, s):
        return remote(sendv.at[r], recvv.at[s], v_send.at[r], v_recv.at[s], r)

    def ask_last():
        return remote(req.at[n - 2], reqlast, last_send.at[0], last_recv.at[0], n - 2)

    def give_edge():
        return remote(
            kv_ref.at[1, pl.ds(0, CMP_STRIDE)], edge, last_send.at[1], last_recv.at[1], n - 2
        )

    def give_last_sum():
        return remote(lastsum, sall.at[n - 2, 1], last_send.at[2], last_recv.at[2], n - 1)

    def give_last_v():
        return remote(sendv.at[0], recvv.at[n - 2], v_send.at[0], v_recv.at[n - 2], n - 1)

    def give_sum(r, s):
        return remote(sall.at[s], sall.at[s], sum_send.at[r], sum_recv.at[s], r)

    def iota(shape, axis):
        return lax.broadcasted_iota(jnp.int32, shape, axis)

    fetches[0].wait()
    fetches[1].wait()
    pl.semaphore_wait(barrier, jnp.where(me < n - 1, 1, 0) + jnp.maximum(me - 1, 0))

    last = n - 1

    @pl.when(me < last)
    def _():
        give_near(0, me + 1).start()

    @pl.when(me < last - 1)
    def _():
        give_near(1, me + 1).start()

    @pl.when(me == last)
    def _():
        give_edge().start()

    lanes = flag.shape[1]
    rows = qblocks * groups

    def column(x, at):
        spot = iota(x.shape, 1) == at
        picked = jnp.sum(jnp.where(spot, x.astype(f32), 0.0), 1, keepdims=True)
        return jnp.broadcast_to(picked, (x.shape[0], QB))

    fetches[2].wait()
    lists = jnp.concatenate([list_ref[b] for b in range(qblocks)], 0)
    lane = iota((rows, lanes), 1)
    member = jnp.zeros((rows, lanes), jnp.int32)
    for i in range(lists.shape[1]):
        member = jnp.where(lists[:, i : i + 1] == lane, 1, member)
    union = member[:groups]
    for b in range(1, qblocks):
        union = jnp.maximum(union, member[b * groups : (b + 1) * groups])
    union = jnp.concatenate([union] * qblocks, 0)
    inner = lane % per
    rank = jnp.zeros_like(union)
    for d in range(1, per):
        rank = rank + jnp.where(inner >= d, pltpu.roll(union, d, 1), 0)

    def first_of(x):
        found = x
        for d in range(1, per):
            found = found + pltpu.roll(x, lanes - d, 1)
        return found

    asked = []
    for j in range(MOST):
        hit = (union == 1) & (rank == j)
        asked.append(first_of(jnp.where(hit, inner, 0))[:groups])
        flag[j * rows : (j + 1) * rows, :] = first_of(jnp.where(hit, member, 0))
    asked = jnp.concatenate(asked, 0)
    low_row = iota((1, WIDE), 1) < DH

    @pl.loop(0, me)
    def _(s):
        ids = column(asked, s * per)
        for j in range(MOST):
            for p in range(slabs):
                at = j * groups + 2 * p
                req[s, j * slabs + p : j * slabs + p + 1, :] = jnp.where(
                    low_row, ids[at : at + 1], ids[at + 1 : at + 2]
                )
        for g in range(groups):
            at = MOST * slabs + g
            req[s, at : at + 1, :] = jnp.where(
                low_row, ids[g : g + 1], ids[groups + g : groups + g + 1]
            )

    @pl.loop(0, me - 1)
    def _(s):
        ask(s, me).start()

    @pl.when(me == last)
    def _():
        ask_last().start()

    for i in range(per):
        own_bias[i] = jnp.where(column(member, me * per + i) > 0.5, 0.0, NEG)
    tri[...] = jnp.where(iota((QB, QB), 0) <= iota((QB, QB), 1), 0.0, NEG)

    def lane_map(shape, source):
        wanted = source(iota((1, shape[1]), 1))
        return jnp.where(iota(shape, 0) == wanted, 1.0, 0.0).astype(bf16)

    half = DH // 2
    partner_map = lane_map((width, width), lambda c: c - c % DH + (c + half) % DH)
    eye = lane_map((width, width), lambda c: c)

    def spread_map(side, turn):
        shape = (per_group * DH, per_group * WIDE)
        return lane_map(
            shape,
            lambda c: jnp.where(
                c % WIDE // DH == side, c // WIDE * DH + (c + turn) % DH, -1
            ),
        )

    def mapped(x, lanes_to):
        return jnp.dot(x, lanes_to, preferred_element_type=f32)

    def score(keys, queries):
        return lax.dot_general(
            keys, queries, (((1,), (1,)), ((), ())), preferred_element_type=f32
        )

    fetches[3].wait()
    fetches[4].wait()
    sign = jnp.where(iota((1, WIDE), 1) % DH < half, -1.0, 1.0)

    def tables(span):
        cos_in, sin_in = base_ref[0], base_ref[1]
        cos_at, sin_at = shift_ref[span, 0:1], shift_ref[span, 1:2]
        cosine = cos_in * cos_at - sin_in * sin_at
        sine = (sin_in * cos_at + cos_in * sin_at) * sign
        return cosine, sine

    def pipelined(steps, ahead, first, second):
        queue = [first(i) for i in range(min(ahead, steps))]
        for i in range(steps):
            if i + ahead < steps:
                queue.append(first(i + ahead))
            second(i, queue.pop(0))

    def turned_slabs(x, cosine, sine):
        other = mapped(x, partner_map)
        found = []
        for p in range(slabs):
            cols = slice(p * WIDE, (p + 1) * WIDE)
            found.append((x[:, cols].astype(f32) * cosine + other[:, cols] * sine).astype(bf16))
        return jnp.concatenate(found, 1)

    cosine, sine = tables(me)
    kt[...] = turned_slabs(kv_ref[0], cosine, sine)

    def flipped(x):
        return score(eye, x).astype(bf16)

    flip = flipped(kv_ref[1])
    for g in range(groups):
        vt[g, :DH] = flip[g * DH : (g + 1) * DH]
        vt[g, DH:] = jnp.ones((ONES, length), bf16)
        svt[g, DH:] = jnp.ones((ONES, n * count), bf16)

    cosine = cosine * scale
    sine = sine * scale
    fetches[5].wait()
    spreads = [(spread_map(side, 0), spread_map(side, half)) for side in range(2)]
    for g in range(groups):
        x = q_ref[:, g * per_group * DH : (g + 1) * per_group * DH]
        plain, other = (mapped(x, lanes_to) for lanes_to in spreads[g % 2])
        for o in range(per_group):
            cols = slice(o * WIDE, (o + 1) * WIDE)
            qraw[g * per_group + o] = plain[:, cols].astype(bf16)
            qt[g * per_group + o] = (plain[:, cols] * cosine + other[:, cols] * sine).astype(bf16)

    def slab_of(h):
        p = h // per_group // 2
        return slice(p * WIDE, (p + 1) * WIDE)

    def own_scores(h):
        return score(kt[:, slab_of(h)], qt[h])

    def own_values(h, raw):
        g = h // per_group
        weights, tops = [], []
        for b in range(qblocks):
            cols = slice(b * QB, (b + 1) * QB)
            parts = []
            for i in range((b + 1) * QB // SLC):
                x = raw[i * SLC : (i + 1) * SLC, cols]
                if i * SLC < b * QB:
                    x = x + own_bias[i, b * groups + g : b * groups + g + 1, :]
                else:
                    x = x + tri[i * SLC - b * QB : (i + 1) * SLC - b * QB, :]
                parts.append(x)
            x = jnp.concatenate(parts, 0)
            peak = jnp.max(x, 0, keepdims=True)
            w = jnp.exp2(x - peak).astype(bf16)
            if x.shape[0] < length:
                w = jnp.concatenate([w, jnp.zeros((length - x.shape[0], QB), bf16)], 0)
            weights.append(w)
            tops.append(peak)
        found = jnp.dot(vt[g], jnp.concatenate(weights, 1), preferred_element_type=f32)
        top[h] = jnp.concatenate(tops, 1)
        total[h] = found[DH : DH + 1]
        acc[h] = found[:DH]

    pipelined(heads, 6, own_scores, own_values)

    fetches[6].wait()
    fetches[7].wait()

    def summarize(w, x, following, p):
        pool = pool_ref[w]
        pool = jnp.concatenate([pool, pool], 1)
        cols = slice(p * WIDE, (p + 1) * WIDE)
        x = x[:, cols].astype(f32)
        after = jnp.concatenate([x[CMP_STRIDE:], following[:, cols].astype(f32)], 0)
        shape = (count, CMP_STRIDE, WIDE)
        z = x.reshape(shape) * pool[None, :CMP_STRIDE] + after.reshape(shape) * pool[None, CMP_STRIDE:]
        found = jnp.sum(z, 1)
        return (found * scale if w == 0 else found).astype(bf16)

    for w in range(2):
        for p in range(slabs):
            sall[me, w, :, p * WIDE : (p + 1) * WIDE] = summarize(
                w, kv_ref[w], jnp.zeros((CMP_STRIDE, width), bf16), p
            )

    def gather(source, w_rows, dst, at):
        for j in range(MOST):
            for p in range(slabs):
                cols = slice(p * WIDE, (p + 1) * WIDE)
                pick = w_rows[j * slabs + p : j * slabs + p + 1, :]
                block = None
                for i in range(per):
                    weight = jnp.broadcast_to(jnp.where(pick == i, 1.0, 0.0), (SLC, WIDE))
                    term = source[i * SLC : (i + 1) * SLC, cols] * weight.astype(bf16)
                    block = term if block is None else block + term
                dst[at, j * SLC : (j + 1) * SLC, cols] = block

    def turned_values(x):
        swapped = [x[(i ^ 1) * SLC : ((i ^ 1) + 1) * SLC] for i in range(per)]
        return score(eye, jnp.concatenate([x, *swapped], 0)).astype(bf16)

    side_row = jnp.where(low_row, 0.0, 1.0)

    def gather_values(flips, w_rows, dst, at):
        for g in range(groups):
            span = slice(g * DH, (g + 1) * DH)
            pick = w_rows[MOST * slabs + g : MOST * slabs + g + 1, :]
            block = None
            for swap in range(2):
                for c in range(per // 2):
                    wanted = jnp.abs(side_row - swap) + 2 * c
                    weight = jnp.broadcast_to(jnp.where(pick == wanted, 1.0, 0.0), (DH, WIDE))
                    start = swap * length + c * WIDE
                    term = flips[span, start : start + WIDE] * weight.astype(bf16)
                    block = term if block is None else block + term
            dst[at, span, :] = block

    def slot_scores(s):
        far_bias[...] = jnp.where(column(flag[...], s * per) > 0.5, 0.0, NEG)

        def first(h):
            return score(recvk[s, :, slab_of(h)], qt[h])

        def second(h, raw):
            g = h // per_group
            rowed = [
                jnp.concatenate(
                    [far_bias[(j * qblocks + b) * groups + g][None] for b in range(qblocks)], 1
                )
                for j in range(MOST)
            ]
            cut = [raw[j * SLC : (j + 1) * SLC] for j in range(MOST)]
            peak = functools.reduce(
                jnp.maximum,
                [jnp.max(x, 0, keepdims=True) + row for x, row in zip(cut, rowed)],
            )
            peak = jnp.maximum(peak, 0.1 * NEG)
            slot_top[s, h] = peak
            for j in range(MOST):
                w = jnp.exp2(cut[j] - (peak - rowed[j])).astype(bf16)
                wslot[s, h, j * SLC : (j + 1) * SLC] = w

        pipelined(heads, 6, first, second)

    def slot_values(s):
        ones = jnp.ones((ONES, size), bf16)

        def first(h):
            g = h // per_group
            values = jnp.concatenate([recvv[s, g * DH : (g + 1) * DH, :], ones], 0)
            return jnp.dot(values, wslot[s, h], preferred_element_type=f32)

        def second(h, found):
            old, fresh = top[h], slot_top[s, h]
            peak = jnp.maximum(old, fresh)
            keep, gain = jnp.exp2(old - peak), jnp.exp2(fresh - peak)
            top[h] = peak
            total[h] = total[h] * keep + found[DH : DH + 1] * gain
            acc[h] = acc[h] * keep + found[:DH] * gain

        pipelined(heads, 4, first, second)

    @pl.when(me == last - 1)
    def _():
        flips = turned_values(kv_ref[1])
        give_edge().wait_recv()
        for p in range(slabs):
            lastsum[:, p * WIDE : (p + 1) * WIDE] = summarize(1, kv_ref[1], edge[...], p)
        ask_last().wait_recv()
        gather_values(flips, reqlast, sendv, 0)
        give_last_sum().start()
        give_last_v().start()

    @pl.when(me >= 1)
    def _():
        s = me - 1
        give_near(0, me).wait_recv()
        turned = turned_slabs(near[0], *tables(s))

        @pl.loop(0, last - me)
        def _(d):
            r = last - d
            ask(s, r).wait_recv()
            gather(turned, reqbuf[r], sendk, r)
            give_k(r, s).start()

        gather(turned, req[s], recvk, s)
        for p in range(slabs):
            sall[s, 0, :, p * WIDE : (p + 1) * WIDE] = summarize(
                0, near[0], kv_ref[0, :CMP_STRIDE], p
            )
        slot_scores(s)

        @pl.when(me < last)
        def _():
            give_near(1, me).wait_recv()
            for p in range(slabs):
                sall[s, 1, :, p * WIDE : (p + 1) * WIDE] = summarize(
                    1, near[1], kv_ref[1, :CMP_STRIDE], p
                )
            flips = turned_values(near[1])

            @pl.loop(0, last - me)
            def _(d):
                r = last - d
                give_sum(r, s).start()
                gather_values(flips, reqbuf[r], sendv, r)
                give_v(r, s).start()

            gather_values(flips, req[s], recvv, s)

        @pl.when(me == last)
        def _():
            give_last_v().wait_recv()

        slot_values(s)

    @pl.loop(0, me - 1)
    def _(s):
        give_k(me, s).wait_recv()
        slot_scores(s)

    @pl.loop(0, me - 1)
    def _(s):
        give_sum(me, s).wait_recv()

    @pl.when(me == last)
    def _():
        give_last_sum().wait_recv()

    blocks = n * count
    known = iota((blocks, width), 0) < (me + 1) * count
    sum_k = jnp.where(known, sall[:, 0].reshape(blocks, width).astype(f32), 0.0).astype(bf16)
    sum_v = jnp.where(known, sall[:, 1].reshape(blocks, width).astype(f32), 0.0).astype(bf16)
    flip = flipped(sum_v)
    for g in range(groups):
        svt[g, :DH] = flip[g * DH : (g + 1) * DH]
    part_at = iota((blocks, length), 0)
    time_at = iota((blocks, length), 1) + me * length
    sbias = jnp.where(part_at * CMP_STRIDE + CMP_BLOCK - 1 <= time_at, 0.0, NEG)

    sks[...] = sum_k

    def summary_scores(h):
        return score(sks[:, slab_of(h)], qraw[h])

    def summary_weights(h, raw):
        x = raw + sbias
        peak = jnp.maximum(jnp.max(x, 0, keepdims=True), 0.1 * NEG)
        wsum[h] = jnp.exp2(x - peak).astype(bf16)

    pipelined(heads, 6, summary_scores, summary_weights)

    def summary_values(h):
        return jnp.dot(svt[h // per_group], wsum[h], preferred_element_type=f32)

    def summary_out(h, found):
        stot[h] = found[DH : DH + 1]
        sacc[h] = found[:DH]

    pipelined(heads, 4, summary_values, summary_out)

    @pl.loop(0, me - 1)
    def _(s):
        give_v(me, s).wait_recv()
        slot_values(s)

    fetches[8].wait()
    fetches[9].wait()
    for pair in range(heads // 2):
        both = []
        for e in range(2):
            h = 2 * pair + e
            first, second = (
                1.0 / (1.0 + jnp.exp(-gate_ref[w, h : h + 1])) for w in range(2)
            )
            mixed = sacc[h] * (first / jnp.maximum(stot[h], 1.0)) + acc[h] * (
                second / total[h]
            )
            mean = jnp.sum(mixed * mixed, 0, keepdims=True) * (1.0 / DH)
            both.append(mixed * lax.rsqrt(mean + EPS))
        cols = slice(pair * WIDE, (pair + 1) * WIDE)
        flat = jnp.concatenate(both, 0).T
        out_ref[0, :, cols] = (flat * gain_ref[:, cols]).astype(bf16)

    @pl.when(me < last)
    def _():
        give_near(0, me + 1).wait_send()

    @pl.when(me < last - 1)
    def _():
        give_near(1, me + 1).wait_send()

    @pl.when(me == last - 1)
    def _():
        give_last_sum().wait_send()
        give_last_v().wait_send()

    @pl.when(me == last)
    def _():
        give_edge().wait_send()
        ask_last().wait_send()

    @pl.loop(0, me - 1)
    def _(s):
        ask(s, me).wait_send()

    @pl.when(me >= 1)
    def _():
        @pl.loop(me + 1, n)
        def _(r):
            give_k(r, me - 1).wait_send()
            give_v(r, me - 1).wait_send()
            give_sum(r, me - 1).wait_send()


def per_device(queries, keys, values, gate_logits, chosen, pool_k, pool_v, out_gain):
    n = lax.axis_size("kv")
    length = queries.shape[1]
    groups = keys.shape[2] // DH
    heads = queries.shape[2] // DH
    qblocks = length // QB
    per = length // SLC
    count = length // CMP_STRIDE
    lanes = -(-n * per // 128) * 128
    rows = qblocks * groups
    width = groups * DH
    size = MOST * SLC
    slabs = groups // 2
    asked = -(-(MOST * slabs + groups) // 8) * 8
    gates = gate_logits.transpose(0, 1, 3, 2)
    base, shift = rope_constants(n, length)
    bf16, f32, i32 = jnp.bfloat16, jnp.float32, jnp.int32
    vm, dma = pltpu.VMEM, pltpu.SemaphoreType.DMA
    scratch = [
        vm((length, heads * DH), bf16),
        vm((2, length, width), bf16),
        vm((2, heads, length), f32),
        vm(chosen.shape[1:], i32),
        vm((2, CMP_BLOCK, DH), f32),
        vm((1, heads * DH), f32),
        vm(base.shape, f32),
        vm(shift.shape, f32),
        vm((2, length, width), bf16),
        vm((heads, length, WIDE), bf16),
        vm((heads, length, WIDE), bf16),
        vm((length, width), bf16),
        vm((groups, DH + ONES, length), bf16),
        vm((n, 2, count, width), bf16),
        vm((n * count, width), bf16),
        vm((groups, DH + ONES, n * count), bf16),
        vm((heads, n * count, length), bf16),
        vm((MOST * rows, lanes), i32),
        vm((per, rows, QB), f32),
        vm((MOST * rows, QB), f32),
        vm((QB, QB), f32),
        vm((n, asked, WIDE), f32),
        vm((n, asked, WIDE), f32),
        vm((asked, WIDE), f32),
        vm((CMP_STRIDE, width), bf16),
        vm((count, width), bf16),
        vm((n, size, width), bf16),
        vm((n, width, size), bf16),
        vm((n, size, width), bf16),
        vm((n, width, size), bf16),
        vm((n, heads, size, length), bf16),
        vm((n, heads, 1, length), f32),
        vm((heads, 1, length), f32),
        vm((heads, 1, length), f32),
        vm((heads, DH, length), f32),
        vm((heads, 1, length), f32),
        vm((heads, DH, length), f32),
        dma((10,)), dma((2,)), dma((2,)),
        dma((n,)), dma((n,)), dma((n,)), dma((n,)), dma((n,)), dma((n,)), dma((n,)), dma((n,)),
        dma((3,)), dma((3,)),
    ]
    operands = (queries, keys, values, gates, chosen, pool_k, pool_v, out_gain[None], base, shift)
    return pl.pallas_call(
        functools.partial(kernel, n),
        out_shape=jax.ShapeDtypeStruct(queries.shape, bf16),
        in_specs=[pl.BlockSpec(memory_space=pltpu.HBM)] * 10,
        out_specs=pl.BlockSpec(memory_space=pltpu.VMEM),
        scratch_shapes=scratch,
        compiler_params=pltpu.CompilerParams(
            collective_id=0, has_side_effects=True, vmem_limit_bytes=44 << 20
        ),
    )(*(pltpu.with_memory_space_constraint(x, pltpu.HBM) for x in operands))


def solution(mesh):
    in_specs = (
        P(("grp", "dp"), "kv", "tp"),
        P(("grp", "dp"), "kv", "tp"),
        P(("grp", "dp"), "kv", "tp"),
        P(("grp", "dp"), None, "kv", "tp"),
        P(("grp", "dp"), "kv", "tp", None),
        P(),
        P(),
        P("tp"),
    )
    out_specs = P(("grp", "dp"), "kv", "tp")
    return jax.shard_map(
        per_device, mesh=mesh, in_specs=in_specs, out_specs=out_specs, check_vma=False
    )
```

```python
import functools

import jax
import jax.numpy as jnp
import numpy as np
from jax import lax
from jax.experimental import pallas as pl
from jax.experimental.pallas import tpu as pltpu
from jax.sharding import PartitionSpec as P

DH = 64
CMP_STRIDE = 16
CMP_BLOCK = 32
SLC = 64
QB = 128
MOST = 2
THETA = 500000.0
EPS = 1e-06
NEG = -1e30
LOG2E = 1.4426950408889634
WIDE = 2 * DH
ONES = 16
MESH = pl.DeviceIdType.MESH


def rope_constants(n, length):
    half = DH // 2
    freq = THETA ** (-2.0 * (np.arange(WIDE) % half) / DH)
    within = np.arange(length)[:, None] * freq[None, :]
    start = np.arange(n)[:, None] * length * freq[None, :]
    base = np.stack([np.cos(within), np.sin(within)]).astype(np.float32)
    shift = np.stack([np.cos(start), np.sin(start)], 1).astype(np.float32)
    return base, shift


def kernel(
    n, q_hbm, k_hbm, v_hbm, gate_hbm, list_hbm, pk_hbm, pv_hbm, gain_hbm, base_hbm, shift_hbm,
    out_ref,
    q_ref, kv_ref, gate_ref, list_ref, pool_ref, gain_ref, base_ref, shift_ref,
    near, qraw, qt, kt, vt, sall, sks, svt, wsum, flag, own_bias, far_bias, tri,
    req, reqbuf, reqlast, edge, lastsum, sendk, sendv, recvk, recvv, wslot, slot_top, slot_total, gain_at,
    top, total, acc, stot, sacc,
    local, near_send, near_recv, req_send, req_recv, k_send, k_recv, v_send, v_recv,
    sum_send, sum_recv, last_send, last_recv,
):
    me = lax.axis_index("kv")
    length = q_ref.shape[0]
    heads = q_ref.shape[1] // DH
    width = kv_ref.shape[2]
    groups = width // DH
    per_group = heads // groups
    pairs = per_group // 2
    slabs = groups // 2
    qblocks = length // QB
    per = length // SLC
    count = length // CMP_STRIDE
    size = MOST * SLC
    scale = DH ** (-0.5) * LOG2E
    f32, bf16 = jnp.float32, jnp.bfloat16

    barrier = pltpu.get_barrier_semaphore()

    @pl.when(me >= 1)
    def _():
        pl.semaphore_signal(barrier, inc=1, device_id={"kv": me - 1}, device_id_type=MESH)

        @pl.loop(me + 1, n)
        def _(r):
            pl.semaphore_signal(barrier, inc=1, device_id={"kv": r}, device_id_type=MESH)

    fetches = [
        pltpu.make_async_copy(src, dst, local.at[i])
        for i, (src, dst) in enumerate(
            (
                (k_hbm.at[0], kv_ref.at[0]),
                (v_hbm.at[0], kv_ref.at[1]),
                (list_hbm.at[0], list_ref),
                (base_hbm, base_ref),
                (shift_hbm, shift_ref),
                (q_hbm.at[0], q_ref),
                (pk_hbm, pool_ref.at[0]),
                (pv_hbm, pool_ref.at[1]),
                (gate_hbm.at[0], gate_ref),
                (gain_hbm, gain_ref),
            )
        )
    ]
    for fetch in fetches:
        fetch.start()

    def remote(src, dst, send, recv, peer):
        return pltpu.make_async_remote_copy(
            src_ref=src, dst_ref=dst, send_sem=send, recv_sem=recv,
            device_id={"kv": peer}, device_id_type=MESH,
        )

    def give_near(w, peer):
        return remote(kv_ref.at[w], near.at[w], near_send.at[w], near_recv.at[w], peer)

    def ask(s, origin):
        return remote(req.at[s], reqbuf.at[origin], req_send.at[s], req_recv.at[origin], s + 1)

    def give_k(r, s):
        return remote(sendk.at[r], recvk.at[s], k_send.at[r], k_recv.at[s], r)

    def give_v(r, s):
        return remote(sendv.at[r], recvv.at[s], v_send.at[r], v_recv.at[s], r)

    def ask_last():
        return remote(req.at[n - 2], reqlast, last_send.at[0], last_recv.at[0], n - 2)

    def give_edge():
        return remote(
            kv_ref.at[1, pl.ds(0, CMP_STRIDE)], edge, last_send.at[1], last_recv.at[1], n - 2
        )

    def give_last_sum():
        return remote(lastsum, sall.at[n - 2, 1], last_send.at[2], last_recv.at[2], n - 1)

    def give_last_v():
        return remote(sendv.at[0], recvv.at[n - 2], v_send.at[0], v_recv.at[n - 2], n - 1)

    def give_sum(r, s):
        return remote(sall.at[s], sall.at[s], sum_send.at[r], sum_recv.at[s], r)

    def iota(shape, axis):
        return lax.broadcasted_iota(jnp.int32, shape, axis)

    fetches[0].wait()
    fetches[1].wait()
    pl.semaphore_wait(barrier, jnp.where(me < n - 1, 1, 0) + jnp.maximum(me - 1, 0))

    last = n - 1

    @pl.when(me < last)
    def _():
        give_near(0, me + 1).start()

    @pl.when(me < last - 1)
    def _():
        give_near(1, me + 1).start()

    @pl.when(me == last)
    def _():
        give_edge().start()

    lanes = flag.shape[1]
    rows = qblocks * groups

    def column(x, at):
        spot = iota(x.shape, 1) == at
        picked = jnp.sum(jnp.where(spot, x.astype(f32), 0.0), 1, keepdims=True)
        return jnp.broadcast_to(picked, (x.shape[0], QB))

    fetches[2].wait()
    lists = jnp.concatenate([list_ref[b] for b in range(qblocks)], 0)
    lane = iota((rows, lanes), 1)
    member = jnp.zeros((rows, lanes), jnp.int32)
    for i in range(lists.shape[1]):
        member = jnp.where(lists[:, i : i + 1] == lane, 1, member)
    union = member[:groups]
    for b in range(1, qblocks):
        union = jnp.maximum(union, member[b * groups : (b + 1) * groups])
    union = jnp.concatenate([union] * qblocks, 0)
    inner = lane % per
    rank = jnp.zeros_like(union)
    for d in range(1, per):
        rank = rank + jnp.where(inner >= d, pltpu.roll(union, d, 1), 0)

    def first_of(x):
        found = x
        for d in range(1, per):
            found = found + pltpu.roll(x, lanes - d, 1)
        return found

    asked = []
    for j in range(MOST):
        hit = (union == 1) & (rank == j)
        asked.append(first_of(jnp.where(hit, inner, 0))[:groups])
        flag[j * rows : (j + 1) * rows, :] = first_of(jnp.where(hit, member, 0))
    asked = jnp.concatenate(asked, 0)
    low_row = iota((1, WIDE), 1) < DH

    @pl.loop(0, me)
    def _(s):
        ids = column(asked, s * per)
        for j in range(MOST):
            for p in range(slabs):
                at = j * groups + 2 * p
                req[s, j * slabs + p : j * slabs + p + 1, :] = jnp.where(
                    low_row, ids[at : at + 1], ids[at + 1 : at + 2]
                )
        for g in range(groups):
            at = MOST * slabs + g
            req[s, at : at + 1, :] = jnp.where(
                low_row, ids[g : g + 1], ids[groups + g : groups + g + 1]
            )

    @pl.loop(0, me - 1)
    def _(s):
        ask(s, me).start()

    @pl.when(me == last)
    def _():
        ask_last().start()

    for i in range(per):
        own_bias[i] = jnp.where(column(member, me * per + i) > 0.5, 0.0, NEG)
    tri[...] = jnp.where(iota((QB, QB), 0) <= iota((QB, QB), 1), 0.0, NEG)

    def lane_map(shape, source):
        wanted = source(iota((1, shape[1]), 1))
        return jnp.where(iota(shape, 0) == wanted, 1.0, 0.0).astype(bf16)

    half = DH // 2
    partner_map = lane_map((width, width), lambda c: c - c % DH + (c + half) % DH)
    eye = lane_map((width, width), lambda c: c)

    def spread_map(side, turn):
        shape = (per_group * DH, per_group * WIDE)
        return lane_map(
            shape,
            lambda c: jnp.where(
                c % WIDE // DH == side, c // WIDE * DH + (c + turn) % DH, -1
            ),
        )

    def mapped(x, lanes_to):
        return jnp.dot(x, lanes_to, preferred_element_type=f32)

    def score(keys, queries):
        return lax.dot_general(
            keys, queries, (((1,), (1,)), ((), ())), preferred_element_type=f32
        )

    fetches[3].wait()
    fetches[4].wait()
    sign = jnp.where(iota((1, WIDE), 1) % DH < half, -1.0, 1.0)

    def tables(span):
        cos_in, sin_in = base_ref[0], base_ref[1]
        cos_at, sin_at = shift_ref[span, 0:1], shift_ref[span, 1:2]
        cosine = cos_in * cos_at - sin_in * sin_at
        sine = (sin_in * cos_at + cos_in * sin_at) * sign
        return cosine, sine

    def pipelined(steps, ahead, first, second):
        queue = [first(i) for i in range(min(ahead, steps))]
        for i in range(steps):
            if i + ahead < steps:
                queue.append(first(i + ahead))
            second(i, queue.pop(0))

    def turned_slabs(x, cosine, sine):
        other = mapped(x, partner_map)
        found = []
        for p in range(slabs):
            cols = slice(p * WIDE, (p + 1) * WIDE)
            found.append((x[:, cols].astype(f32) * cosine + other[:, cols] * sine).astype(bf16))
        return jnp.concatenate(found, 1)

    cosine, sine = tables(me)
    kt[...] = turned_slabs(kv_ref[0], cosine, sine)

    def flipped(x):
        return score(eye, x).astype(bf16)

    flip = flipped(kv_ref[1])
    for g in range(groups):
        vt[g, :DH] = flip[g * DH : (g + 1) * DH]
        vt[g, DH:] = jnp.ones((ONES, length), bf16)
        svt[g, DH:] = jnp.ones((ONES, n * count), bf16)

    cosine = cosine * scale
    sine = sine * scale
    fetches[5].wait()
    spreads = [(spread_map(side, 0), spread_map(side, half)) for side in range(2)]
    for g in range(groups):
        x = q_ref[:, g * per_group * DH : (g + 1) * per_group * DH]
        plain, other = (mapped(x, lanes_to) for lanes_to in spreads[g % 2])
        for o in range(per_group):
            cols = slice(o * WIDE, (o + 1) * WIDE)
            qraw[g * per_group + o] = plain[:, cols].astype(bf16)
            qt[g * per_group + o] = (plain[:, cols] * cosine + other[:, cols] * sine).astype(bf16)

    def slab_of(h):
        p = h // per_group // 2
        return slice(p * WIDE, (p + 1) * WIDE)

    def own_scores(h):
        return score(kt[:, slab_of(h)], qt[h])

    def own_values(h, raw):
        g = h // per_group
        weights, tops = [], []
        for b in range(qblocks):
            cols = slice(b * QB, (b + 1) * QB)
            parts = []
            for i in range((b + 1) * QB // SLC):
                x = raw[i * SLC : (i + 1) * SLC, cols]
                if i * SLC < b * QB:
                    x = x + own_bias[i, b * groups + g : b * groups + g + 1, :]
                else:
                    x = x + tri[i * SLC - b * QB : (i + 1) * SLC - b * QB, :]
                parts.append(x)
            x = jnp.concatenate(parts, 0)
            peak = jnp.max(x, 0, keepdims=True)
            w = jnp.exp2(x - peak).astype(bf16)
            if x.shape[0] < length:
                w = jnp.concatenate([w, jnp.zeros((length - x.shape[0], QB), bf16)], 0)
            weights.append(w)
            tops.append(peak)
        found = jnp.dot(vt[g], jnp.concatenate(weights, 1), preferred_element_type=f32)
        top[h : h + 1] = jnp.concatenate(tops, 1)
        total[h : h + 1] = found[DH : DH + 1]
        acc[h] = found[:DH]

    pipelined(heads, 6, own_scores, own_values)

    fetches[9].wait()
    for pair in range(heads // 2):
        row = gain_ref[:, pair * WIDE : (pair + 1) * WIDE]
        gain_at[pair] = jnp.broadcast_to(row, (WIDE, WIDE)).T

    fetches[6].wait()
    fetches[7].wait()

    def summarize(w, x, following, p):
        pool = pool_ref[w]
        pool = jnp.concatenate([pool, pool], 1)
        cols = slice(p * WIDE, (p + 1) * WIDE)
        x = x[:, cols].astype(f32)
        after = jnp.concatenate([x[CMP_STRIDE:], following[:, cols].astype(f32)], 0)
        shape = (count, CMP_STRIDE, WIDE)
        z = x.reshape(shape) * pool[None, :CMP_STRIDE] + after.reshape(shape) * pool[None, CMP_STRIDE:]
        found = jnp.sum(z, 1)
        return (found * scale if w == 0 else found).astype(bf16)

    for w in range(2):
        for p in range(slabs):
            sall[me, w, :, p * WIDE : (p + 1) * WIDE] = summarize(
                w, kv_ref[w], jnp.zeros((CMP_STRIDE, width), bf16), p
            )

    def gather(source, w_rows, dst, at):
        for j in range(MOST):
            for p in range(slabs):
                cols = slice(p * WIDE, (p + 1) * WIDE)
                pick = w_rows[j * slabs + p : j * slabs + p + 1, :]
                block = None
                for i in range(per):
                    weight = jnp.broadcast_to(jnp.where(pick == i, 1.0, 0.0), (SLC, WIDE))
                    term = source[i * SLC : (i + 1) * SLC, cols] * weight.astype(bf16)
                    block = term if block is None else block + term
                dst[at, j * SLC : (j + 1) * SLC, cols] = block

    def turned_values(x):
        swapped = [x[(i ^ 1) * SLC : ((i ^ 1) + 1) * SLC] for i in range(per)]
        return score(eye, jnp.concatenate([x, *swapped], 0)).astype(bf16)

    side_row = jnp.where(low_row, 0.0, 1.0)

    def gather_values(flips, w_rows, dst, at):
        for g in range(groups):
            span = slice(g * DH, (g + 1) * DH)
            pick = w_rows[MOST * slabs + g : MOST * slabs + g + 1, :]
            block = None
            for swap in range(2):
                for c in range(per // 2):
                    wanted = jnp.abs(side_row - swap) + 2 * c
                    weight = jnp.broadcast_to(jnp.where(pick == wanted, 1.0, 0.0), (DH, WIDE))
                    start = swap * length + c * WIDE
                    term = flips[span, start : start + WIDE] * weight.astype(bf16)
                    block = term if block is None else block + term
            dst[at, span, :] = block

    def slot_scores(s):
        far_bias[...] = jnp.where(column(flag[...], s * per) > 0.5, 0.0, NEG)

        def first(h):
            return score(recvk[s, :, slab_of(h)], qt[h])

        def second(h, raw):
            g = h // per_group
            rowed = [
                jnp.concatenate(
                    [far_bias[(j * qblocks + b) * groups + g][None] for b in range(qblocks)], 1
                )
                for j in range(MOST)
            ]
            cut = [raw[j * SLC : (j + 1) * SLC] for j in range(MOST)]
            peak = functools.reduce(
                jnp.maximum,
                [jnp.max(x, 0, keepdims=True) + row for x, row in zip(cut, rowed)],
            )
            peak = jnp.maximum(peak, 0.1 * NEG)
            slot_top[s, h : h + 1] = peak
            sums = []
            for j in range(MOST):
                w = jnp.exp2(cut[j] - (peak - rowed[j]))
                sums.append(jnp.sum(w, 0, keepdims=True))
                wslot[s, h, j * SLC : (j + 1) * SLC] = w.astype(bf16)
            slot_total[s, h : h + 1] = functools.reduce(jnp.add, sums)

        pipelined(heads, 6, first, second)

    def slot_product(s, h):
        g = h // per_group
        return jnp.dot(
            recvv[s, g * DH : (g + 1) * DH, :], wslot[s, h], preferred_element_type=f32
        )

    def slot_values(s):
        old, fresh = top[...], slot_top[s]
        peak = jnp.maximum(old, fresh)
        keep, gain = jnp.exp2(old - peak), jnp.exp2(fresh - peak)
        top[...] = peak
        total[...] = total[...] * keep + slot_total[s] * gain

        def second(h, found):
            acc[h] = acc[h] * keep[h : h + 1] + found * gain[h : h + 1]

        pipelined(heads, 4, lambda h: slot_product(s, h), second)

    @pl.when(me == last - 1)
    def _():
        flips = turned_values(kv_ref[1])
        give_edge().wait_recv()
        for p in range(slabs):
            lastsum[:, p * WIDE : (p + 1) * WIDE] = summarize(1, kv_ref[1], edge[...], p)
        ask_last().wait_recv()
        gather_values(flips, reqlast, sendv, 0)
        give_last_sum().start()
        give_last_v().start()

    @pl.when(me >= 1)
    def _():
        s = me - 1
        give_near(0, me).wait_recv()
        turned = turned_slabs(near[0], *tables(s))

        @pl.loop(0, last - me)
        def _(d):
            r = last - d
            ask(s, r).wait_recv()
            gather(turned, reqbuf[r], sendk, r)
            give_k(r, s).start()

        gather(turned, req[s], recvk, s)
        for p in range(slabs):
            sall[s, 0, :, p * WIDE : (p + 1) * WIDE] = summarize(
                0, near[0], kv_ref[0, :CMP_STRIDE], p
            )
        slot_scores(s)

        @pl.when(me < last)
        def _():
            give_near(1, me).wait_recv()
            for p in range(slabs):
                sall[s, 1, :, p * WIDE : (p + 1) * WIDE] = summarize(
                    1, near[1], kv_ref[1, :CMP_STRIDE], p
                )

            @pl.loop(me + 1, n)
            def _(r):
                give_sum(r, s).start()

            flips = turned_values(near[1])

            @pl.loop(0, last - me)
            def _(d):
                r = last - d
                gather_values(flips, reqbuf[r], sendv, r)
                give_v(r, s).start()

            gather_values(flips, req[s], recvv, s)

        @pl.when(me == last)
        def _():
            give_last_v().wait_recv()

        slot_values(s)

    @pl.loop(0, me - 1)
    def _(s):
        give_k(me, s).wait_recv()
        slot_scores(s)

    @pl.loop(0, me - 1)
    def _(s):
        give_sum(me, s).wait_recv()

    @pl.when(me == last)
    def _():
        give_last_sum().wait_recv()

    blocks = n * count
    known = iota((blocks, width), 0) < (me + 1) * count
    sum_k = jnp.where(known, sall[:, 0].reshape(blocks, width).astype(f32), 0.0).astype(bf16)
    sum_v = jnp.where(known, sall[:, 1].reshape(blocks, width).astype(f32), 0.0).astype(bf16)
    flip = flipped(sum_v)
    for g in range(groups):
        svt[g, :DH] = flip[g * DH : (g + 1) * DH]
    part_at = iota((blocks, length), 0)
    time_at = iota((blocks, length), 1) + me * length
    sbias = jnp.where(part_at * CMP_STRIDE + CMP_BLOCK - 1 <= time_at, 0.0, NEG)

    sks[...] = sum_k

    def summary_scores(h):
        return score(sks[:, slab_of(h)], qraw[h])

    def summary_weights(h, raw):
        x = raw + sbias
        peak = jnp.maximum(jnp.max(x, 0, keepdims=True), 0.1 * NEG)
        wsum[h] = jnp.exp2(x - peak).astype(bf16)

    pipelined(heads, 6, summary_scores, summary_weights)

    def summary_values(h):
        return jnp.dot(svt[h // per_group], wsum[h], preferred_element_type=f32)

    def summary_out(h, found):
        stot[h : h + 1] = found[DH : DH + 1]
        sacc[h] = found[:DH]

    pipelined(heads, 4, summary_values, summary_out)

    fetches[8].wait()
    first_gate, second_gate = (1.0 / (1.0 + jnp.exp(-gate_ref[w])) for w in range(2))
    far = jnp.maximum(me - 1, 0)
    peak = lax.fori_loop(0, far, lambda s, x: jnp.maximum(x, slot_top[s]), top[...])
    keep = jnp.exp2(top[...] - peak)
    whole = lax.fori_loop(
        0,
        far,
        lambda s, x: x + slot_total[s] * jnp.exp2(slot_top[s] - peak),
        total[...] * keep,
    )
    shared = second_gate / whole
    keep = keep * shared
    first_gate = first_gate / jnp.maximum(stot[...], 1.0)

    @pl.loop(0, me - 1)
    def _(s):
        slot_top[s] = jnp.exp2(slot_top[s] - peak) * shared

    for h in range(heads):
        acc[h] = sacc[h] * first_gate[h : h + 1] + acc[h] * keep[h : h + 1]

    @pl.loop(0, me - 1)
    def _(s):
        give_v(me, s).wait_recv()

        def second(h, found):
            acc[h] = acc[h] + found * slot_top[s, h : h + 1]

        pipelined(heads, 4, lambda h: slot_product(s, h), second)

    for pair in range(heads // 2):
        both = []
        for e in range(2):
            mixed = acc[2 * pair + e]
            mean = jnp.sum(mixed * mixed, 0, keepdims=True) * (1.0 / DH)
            both.append(mixed * lax.rsqrt(mean + EPS))
        flat = jnp.concatenate(both, 0) * jnp.concatenate([gain_at[pair]] * (length // WIDE), 1)
        out_ref[0, :, pair * WIDE : (pair + 1) * WIDE] = flat.astype(bf16).T

    @pl.when(me < last)
    def _():
        give_near(0, me + 1).wait_send()

    @pl.when(me < last - 1)
    def _():
        give_near(1, me + 1).wait_send()

    @pl.when(me == last - 1)
    def _():
        give_last_sum().wait_send()
        give_last_v().wait_send()

    @pl.when(me == last)
    def _():
        give_edge().wait_send()
        ask_last().wait_send()

    @pl.loop(0, me - 1)
    def _(s):
        ask(s, me).wait_send()

    @pl.when(me >= 1)
    def _():
        @pl.loop(me + 1, n)
        def _(r):
            give_k(r, me - 1).wait_send()
            give_v(r, me - 1).wait_send()
            give_sum(r, me - 1).wait_send()


def per_device(queries, keys, values, gate_logits, chosen, pool_k, pool_v, out_gain):
    n = lax.axis_size("kv")
    length = queries.shape[1]
    groups = keys.shape[2] // DH
    heads = queries.shape[2] // DH
    qblocks = length // QB
    per = length // SLC
    count = length // CMP_STRIDE
    lanes = -(-n * per // 128) * 128
    rows = qblocks * groups
    width = groups * DH
    size = MOST * SLC
    slabs = groups // 2
    asked = -(-(MOST * slabs + groups) // 8) * 8
    gates = gate_logits.transpose(0, 1, 3, 2)
    base, shift = rope_constants(n, length)
    bf16, f32, i32 = jnp.bfloat16, jnp.float32, jnp.int32
    vm, dma = pltpu.VMEM, pltpu.SemaphoreType.DMA
    scratch = [
        vm((length, heads * DH), bf16),
        vm((2, length, width), bf16),
        vm((2, heads, length), f32),
        vm(chosen.shape[1:], i32),
        vm((2, CMP_BLOCK, DH), f32),
        vm((1, heads * DH), f32),
        vm(base.shape, f32),
        vm(shift.shape, f32),
        vm((2, length, width), bf16),
        vm((heads, length, WIDE), bf16),
        vm((heads, length, WIDE), bf16),
        vm((length, width), bf16),
        vm((groups, DH + ONES, length), bf16),
        vm((n, 2, count, width), bf16),
        vm((n * count, width), bf16),
        vm((groups, DH + ONES, n * count), bf16),
        vm((heads, n * count, length), bf16),
        vm((MOST * rows, lanes), i32),
        vm((per, rows, QB), f32),
        vm((MOST * rows, QB), f32),
        vm((QB, QB), f32),
        vm((n, asked, WIDE), f32),
        vm((n, asked, WIDE), f32),
        vm((asked, WIDE), f32),
        vm((CMP_STRIDE, width), bf16),
        vm((count, width), bf16),
        vm((n, size, width), bf16),
        vm((n, width, size), bf16),
        vm((n, size, width), bf16),
        vm((n, width, size), bf16),
        vm((n, heads, size, length), bf16),
        vm((n, heads, length), f32),
        vm((n, heads, length), f32),
        vm((heads // 2, WIDE, WIDE), f32),
        vm((heads, length), f32),
        vm((heads, length), f32),
        vm((heads, DH, length), f32),
        vm((heads, length), f32),
        vm((heads, DH, length), f32),
        dma((10,)), dma((2,)), dma((2,)),
        dma((n,)), dma((n,)), dma((n,)), dma((n,)), dma((n,)), dma((n,)), dma((n,)), dma((n,)),
        dma((3,)), dma((3,)),
    ]
    operands = (queries, keys, values, gates, chosen, pool_k, pool_v, out_gain[None], base, shift)
    return pl.pallas_call(
        functools.partial(kernel, n),
        out_shape=jax.ShapeDtypeStruct(queries.shape, bf16),
        in_specs=[pl.BlockSpec(memory_space=pltpu.HBM)] * 10,
        out_specs=pl.BlockSpec(memory_space=pltpu.VMEM),
        scratch_shapes=scratch,
        compiler_params=pltpu.CompilerParams(
            collective_id=0, has_side_effects=True, vmem_limit_bytes=44 << 20
        ),
    )(*(pltpu.with_memory_space_constraint(x, pltpu.HBM) for x in operands))


def solution(mesh):
    in_specs = (
        P(("grp", "dp"), "kv", "tp"),
        P(("grp", "dp"), "kv", "tp"),
        P(("grp", "dp"), "kv", "tp"),
        P(("grp", "dp"), None, "kv", "tp"),
        P(("grp", "dp"), "kv", "tp", None),
        P(),
        P(),
        P("tp"),
    )
    out_specs = P(("grp", "dp"), "kv", "tp")
    return jax.shard_map(
        per_device, mesh=mesh, in_specs=in_specs, out_specs=out_specs, check_vma=False
    )
```

```python
import functools

import jax
import jax.numpy as jnp
import numpy as np
from jax import lax
from jax.experimental import pallas as pl
from jax.experimental.pallas import tpu as pltpu
from jax.sharding import PartitionSpec as P

DH = 64
CMP_STRIDE = 16
CMP_BLOCK = 32
SLC = 64
QB = 128
MOST = 2
THETA = 500000.0
EPS = 1e-06
NEG = -1e30
LOG2E = 1.4426950408889634
WIDE = 2 * DH
ONES = 16
MESH = pl.DeviceIdType.MESH


def rope_constants(n, length):
    half = DH // 2
    freq = THETA ** (-2.0 * (np.arange(WIDE) % half) / DH)
    within = np.arange(length)[:, None] * freq[None, :]
    start = np.arange(n)[:, None] * length * freq[None, :]
    base = np.stack([np.cos(within), np.sin(within)]).astype(np.float32)
    shift = np.stack([np.cos(start), np.sin(start)], 1).astype(np.float32)
    return base, shift


def kernel(
    n, q_hbm, k_hbm, v_hbm, gate_hbm, list_hbm, pk_hbm, pv_hbm, gain_hbm, base_hbm, shift_hbm,
    out_ref,
    q_ref, kv_ref, gate_ref, list_ref, pool_ref, gain_ref, base_ref, shift_ref,
    near, qraw, qt, kt, vt, sall, sks, svt, wsum, flag, own_bias, far_bias, tri,
    req, reqbuf, reqlast, edge, lastsum, sendk, sendv, recvk, recvv, wslot, slot_top, slot_total, gain_at,
    top, total, acc, stot, sacc,
    local, near_send, near_recv, req_send, req_recv, k_send, k_recv, v_send, v_recv,
    sum_send, sum_recv, last_send, last_recv,
):
    me = lax.axis_index("kv")
    length = q_ref.shape[0]
    heads = q_ref.shape[1] // DH
    width = kv_ref.shape[2]
    groups = width // DH
    per_group = heads // groups
    pairs = per_group // 2
    slabs = groups // 2
    qblocks = length // QB
    per = length // SLC
    count = length // CMP_STRIDE
    size = MOST * SLC
    scale = DH ** (-0.5) * LOG2E
    f32, bf16 = jnp.float32, jnp.bfloat16

    barrier = pltpu.get_barrier_semaphore()

    @pl.when(me >= 1)
    def _():
        pl.semaphore_signal(barrier, inc=1, device_id={"kv": me - 1}, device_id_type=MESH)

        @pl.loop(me + 1, n)
        def _(r):
            pl.semaphore_signal(barrier, inc=1, device_id={"kv": r}, device_id_type=MESH)

    fetches = [
        pltpu.make_async_copy(src, dst, local.at[i])
        for i, (src, dst) in enumerate(
            (
                (k_hbm.at[0], kv_ref.at[0]),
                (v_hbm.at[0], kv_ref.at[1]),
                (list_hbm.at[0], list_ref),
                (base_hbm, base_ref),
                (shift_hbm, shift_ref),
                (q_hbm.at[0], q_ref),
                (pk_hbm, pool_ref.at[0]),
                (pv_hbm, pool_ref.at[1]),
                (gate_hbm.at[0], gate_ref),
                (gain_hbm, gain_ref),
            )
        )
    ]
    for fetch in fetches:
        fetch.start()

    def remote(src, dst, send, recv, peer):
        return pltpu.make_async_remote_copy(
            src_ref=src, dst_ref=dst, send_sem=send, recv_sem=recv,
            device_id={"kv": peer}, device_id_type=MESH,
        )

    def give_near(w, peer):
        return remote(kv_ref.at[w], near.at[w], near_send.at[w], near_recv.at[w], peer)

    def ask(s, origin):
        return remote(req.at[s], reqbuf.at[origin], req_send.at[s], req_recv.at[origin], s + 1)

    def give_k(r, s):
        return remote(sendk.at[r], recvk.at[s], k_send.at[r], k_recv.at[s], r)

    def give_v(r, s):
        return remote(sendv.at[r], recvv.at[s], v_send.at[r], v_recv.at[s], r)

    def ask_last():
        return remote(req.at[n - 2], reqlast, last_send.at[0], last_recv.at[0], n - 2)

    def give_edge():
        return remote(
            kv_ref.at[1, pl.ds(0, CMP_STRIDE)], edge, last_send.at[1], last_recv.at[1], n - 2
        )

    def give_last_sum():
        return remote(lastsum, sall.at[n - 2, 1], last_send.at[2], last_recv.at[2], n - 1)

    def give_last_v():
        return remote(sendv.at[0], recvv.at[n - 2], v_send.at[0], v_recv.at[n - 2], n - 1)

    def give_sum(r, s):
        return remote(sall.at[s], sall.at[s], sum_send.at[r], sum_recv.at[s], r)

    def iota(shape, axis):
        return lax.broadcasted_iota(jnp.int32, shape, axis)

    fetches[0].wait()
    fetches[1].wait()
    pl.semaphore_wait(barrier, jnp.where(me < n - 1, 1, 0) + jnp.maximum(me - 1, 0))

    last = n - 1

    @pl.when(me < last)
    def _():
        give_near(0, me + 1).start()

    @pl.when(me < last - 1)
    def _():
        give_near(1, me + 1).start()

    @pl.when(me == last)
    def _():
        give_edge().start()

    lanes = flag.shape[1]
    rows = qblocks * groups

    def column(x, at):
        spot = iota(x.shape, 1) == at
        picked = jnp.sum(jnp.where(spot, x.astype(f32), 0.0), 1, keepdims=True)
        return jnp.broadcast_to(picked, (x.shape[0], QB))

    fetches[2].wait()
    lists = jnp.concatenate([list_ref[b] for b in range(qblocks)], 0)
    lane = iota((rows, lanes), 1)
    member = jnp.zeros((rows, lanes), jnp.int32)
    for i in range(lists.shape[1]):
        member = jnp.where(lists[:, i : i + 1] == lane, 1, member)
    union = member[:groups]
    for b in range(1, qblocks):
        union = jnp.maximum(union, member[b * groups : (b + 1) * groups])
    union = jnp.concatenate([union] * qblocks, 0)
    inner = lane % per
    rank = jnp.zeros_like(union)
    for d in range(1, per):
        rank = rank + jnp.where(inner >= d, pltpu.roll(union, d, 1), 0)

    def first_of(x):
        found = x
        for d in range(1, per):
            found = found + pltpu.roll(x, lanes - d, 1)
        return found

    asked = []
    for j in range(MOST):
        hit = (union == 1) & (rank == j)
        asked.append(first_of(jnp.where(hit, inner, 0))[:groups])
        flag[j * rows : (j + 1) * rows, :] = first_of(jnp.where(hit, member, 0))
    asked = jnp.concatenate(asked, 0)
    low_row = iota((1, WIDE), 1) < DH

    @pl.loop(0, me)
    def _(s):
        ids = column(asked, s * per)
        for j in range(MOST):
            for p in range(slabs):
                at = j * groups + 2 * p
                req[s, j * slabs + p : j * slabs + p + 1, :] = jnp.where(
                    low_row, ids[at : at + 1], ids[at + 1 : at + 2]
                )
        for g in range(groups):
            at = MOST * slabs + g
            req[s, at : at + 1, :] = jnp.where(
                low_row, ids[g : g + 1], ids[groups + g : groups + g + 1]
            )

    @pl.loop(0, me - 1)
    def _(s):
        ask(s, me).start()

    @pl.when(me == last)
    def _():
        ask_last().start()

    for i in range(per):
        own_bias[i] = jnp.where(column(member, me * per + i) > 0.5, 0.0, NEG)
    tri[...] = jnp.where(iota((QB, QB), 0) <= iota((QB, QB), 1), 0.0, NEG)

    def lane_map(shape, source):
        wanted = source(iota((1, shape[1]), 1))
        return jnp.where(iota(shape, 0) == wanted, 1.0, 0.0).astype(bf16)

    half = DH // 2
    partner_map = lane_map((width, width), lambda c: c - c % DH + (c + half) % DH)
    eye = lane_map((width, width), lambda c: c)

    def spread_map(side, turn):
        shape = (per_group * DH, per_group * WIDE)
        return lane_map(
            shape,
            lambda c: jnp.where(
                c % WIDE // DH == side, c // WIDE * DH + (c + turn) % DH, -1
            ),
        )

    def mapped(x, lanes_to):
        return jnp.dot(x, lanes_to, preferred_element_type=f32)

    def score(keys, queries):
        return lax.dot_general(
            keys, queries, (((1,), (1,)), ((), ())), preferred_element_type=f32
        )

    fetches[3].wait()
    fetches[4].wait()
    sign = jnp.where(iota((1, WIDE), 1) % DH < half, -1.0, 1.0)

    def tables(span):
        cos_in, sin_in = base_ref[0], base_ref[1]
        cos_at, sin_at = shift_ref[span, 0:1], shift_ref[span, 1:2]
        cosine = cos_in * cos_at - sin_in * sin_at
        sine = (sin_in * cos_at + cos_in * sin_at) * sign
        return cosine, sine

    def pipelined(steps, ahead, first, second):
        queue = [first(i) for i in range(min(ahead, steps))]
        for i in range(steps):
            if i + ahead < steps:
                queue.append(first(i + ahead))
            second(i, queue.pop(0))

    def turned_slabs(x, cosine, sine):
        other = mapped(x, partner_map)
        found = []
        for p in range(slabs):
            cols = slice(p * WIDE, (p + 1) * WIDE)
            found.append((x[:, cols].astype(f32) * cosine + other[:, cols] * sine).astype(bf16))
        return jnp.concatenate(found, 1)

    cosine, sine = tables(me)
    kt[...] = turned_slabs(kv_ref[0], cosine, sine)

    def flipped(x):
        return score(eye, x).astype(bf16)

    flip = flipped(kv_ref[1])
    for g in range(groups):
        vt[g, :DH] = flip[g * DH : (g + 1) * DH]
        vt[g, DH:] = jnp.ones((ONES, length), bf16)
        svt[g, DH:] = jnp.ones((ONES, n * count), bf16)

    cosine = cosine * scale
    sine = sine * scale
    fetches[5].wait()
    spreads = [(spread_map(side, 0), spread_map(side, half)) for side in range(2)]
    for g in range(groups):
        x = q_ref[:, g * per_group * DH : (g + 1) * per_group * DH]
        plain, other = (mapped(x, lanes_to) for lanes_to in spreads[g % 2])
        for o in range(per_group):
            cols = slice(o * WIDE, (o + 1) * WIDE)
            qraw[g * per_group + o] = plain[:, cols].astype(bf16)
            qt[g * per_group + o] = (plain[:, cols] * cosine + other[:, cols] * sine).astype(bf16)

    def slab_of(h):
        p = h // per_group // 2
        return slice(p * WIDE, (p + 1) * WIDE)

    def own_scores(h):
        return score(kt[:, slab_of(h)], qt[h])

    def own_values(h, raw):
        g = h // per_group
        weights, tops = [], []
        for b in range(qblocks):
            cols = slice(b * QB, (b + 1) * QB)
            parts = []
            for i in range((b + 1) * QB // SLC):
                x = raw[i * SLC : (i + 1) * SLC, cols]
                if i * SLC < b * QB:
                    x = x + own_bias[i, b * groups + g : b * groups + g + 1, :]
                else:
                    x = x + tri[i * SLC - b * QB : (i + 1) * SLC - b * QB, :]
                parts.append(x)
            x = jnp.concatenate(parts, 0)
            peak = jnp.max(x, 0, keepdims=True)
            w = jnp.exp2(x - peak).astype(bf16)
            if x.shape[0] < length:
                w = jnp.concatenate([w, jnp.zeros((length - x.shape[0], QB), bf16)], 0)
            weights.append(w)
            tops.append(peak)
        found = jnp.dot(vt[g], jnp.concatenate(weights, 1), preferred_element_type=f32)
        top[h : h + 1] = jnp.concatenate(tops, 1)
        total[h : h + 1] = found[DH : DH + 1]
        acc[h] = found[:DH]

    pipelined(heads, 6, own_scores, own_values)

    fetches[9].wait()
    for pair in range(heads // 2):
        row = gain_ref[:, pair * WIDE : (pair + 1) * WIDE]
        gain_at[pair] = jnp.broadcast_to(row, (WIDE, WIDE)).T

    fetches[6].wait()
    fetches[7].wait()

    def summarize(w, x, following, p):
        pool = pool_ref[w]
        pool = jnp.concatenate([pool, pool], 1)
        cols = slice(p * WIDE, (p + 1) * WIDE)
        x = x[:, cols].astype(f32)
        after = jnp.concatenate([x[CMP_STRIDE:], following[:, cols].astype(f32)], 0)
        shape = (count, CMP_STRIDE, WIDE)
        z = x.reshape(shape) * pool[None, :CMP_STRIDE] + after.reshape(shape) * pool[None, CMP_STRIDE:]
        found = jnp.sum(z, 1)
        return (found * scale if w == 0 else found).astype(bf16)

    for w in range(2):
        for p in range(slabs):
            sall[me, w, :, p * WIDE : (p + 1) * WIDE] = summarize(
                w, kv_ref[w], jnp.zeros((CMP_STRIDE, width), bf16), p
            )

    def gather(source, w_rows, dst, at):
        for j in range(MOST):
            for p in range(slabs):
                cols = slice(p * WIDE, (p + 1) * WIDE)
                pick = w_rows[j * slabs + p : j * slabs + p + 1, :]
                block = None
                for i in range(per):
                    weight = jnp.broadcast_to(jnp.where(pick == i, 1.0, 0.0), (SLC, WIDE))
                    term = source[i * SLC : (i + 1) * SLC, cols] * weight.astype(bf16)
                    block = term if block is None else block + term
                dst[at, j * SLC : (j + 1) * SLC, cols] = block

    def turned_values(x):
        swapped = [x[(i ^ 1) * SLC : ((i ^ 1) + 1) * SLC] for i in range(per)]
        return score(eye, jnp.concatenate([x, *swapped], 0)).astype(bf16)

    side_row = jnp.where(low_row, 0.0, 1.0)

    def gather_values(flips, w_rows, dst, at):
        for g in range(groups):
            span = slice(g * DH, (g + 1) * DH)
            pick = w_rows[MOST * slabs + g : MOST * slabs + g + 1, :]
            block = None
            for swap in range(2):
                for c in range(per // 2):
                    wanted = jnp.abs(side_row - swap) + 2 * c
                    weight = jnp.broadcast_to(jnp.where(pick == wanted, 1.0, 0.0), (DH, WIDE))
                    start = swap * length + c * WIDE
                    term = flips[span, start : start + WIDE] * weight.astype(bf16)
                    block = term if block is None else block + term
            dst[at, span, :] = block

    def slot_scores(s):
        far_bias[...] = jnp.where(column(flag[...], s * per) > 0.5, 0.0, NEG)

        def first(h):
            return score(recvk[s, :, slab_of(h)], qt[h])

        def second(h, raw):
            g = h // per_group
            rowed = [
                jnp.concatenate(
                    [far_bias[(j * qblocks + b) * groups + g][None] for b in range(qblocks)], 1
                )
                for j in range(MOST)
            ]
            cut = [raw[j * SLC : (j + 1) * SLC] for j in range(MOST)]
            peak = functools.reduce(
                jnp.maximum,
                [jnp.max(x, 0, keepdims=True) + row for x, row in zip(cut, rowed)],
            )
            peak = jnp.maximum(peak, 0.1 * NEG)
            slot_top[s, h : h + 1] = peak
            sums = []
            for j in range(MOST):
                w = jnp.exp2(cut[j] - (peak - rowed[j]))
                sums.append(jnp.sum(w, 0, keepdims=True))
                wslot[s, h, j * SLC : (j + 1) * SLC] = w.astype(bf16)
            slot_total[s, h : h + 1] = functools.reduce(jnp.add, sums)

        pipelined(heads, 6, first, second)

    def slot_product(s, h):
        g = h // per_group
        return jnp.dot(
            recvv[s, g * DH : (g + 1) * DH, :], wslot[s, h], preferred_element_type=f32
        )

    def slot_values(s):
        old, fresh = top[...], slot_top[s]
        peak = jnp.maximum(old, fresh)
        keep, gain = jnp.exp2(old - peak), jnp.exp2(fresh - peak)
        top[...] = peak
        total[...] = total[...] * keep + slot_total[s] * gain

        def second(h, found):
            acc[h] = acc[h] * keep[h : h + 1] + found * gain[h : h + 1]

        pipelined(heads, 4, lambda h: slot_product(s, h), second)

    @pl.when(me == last - 1)
    def _():
        flips = turned_values(kv_ref[1])
        give_edge().wait_recv()
        for p in range(slabs):
            lastsum[:, p * WIDE : (p + 1) * WIDE] = summarize(1, kv_ref[1], edge[...], p)
        ask_last().wait_recv()
        gather_values(flips, reqlast, sendv, 0)
        give_last_sum().start()
        give_last_v().start()

    @pl.when(me >= 1)
    def _():
        s = me - 1
        give_near(0, me).wait_recv()
        turned = turned_slabs(near[0], *tables(s))

        @pl.loop(0, last - me)
        def _(d):
            r = last - d
            ask(s, r).wait_recv()
            gather(turned, reqbuf[r], sendk, r)
            give_k(r, s).start()

        gather(turned, req[s], recvk, s)
        for p in range(slabs):
            sall[s, 0, :, p * WIDE : (p + 1) * WIDE] = summarize(
                0, near[0], kv_ref[0, :CMP_STRIDE], p
            )
        slot_scores(s)

        @pl.when(me < last)
        def _():
            give_near(1, me).wait_recv()
            for p in range(slabs):
                sall[s, 1, :, p * WIDE : (p + 1) * WIDE] = summarize(
                    1, near[1], kv_ref[1, :CMP_STRIDE], p
                )

            @pl.loop(me + 1, n)
            def _(r):
                give_sum(r, s).start()

            flips = turned_values(near[1])

            @pl.loop(me + 1, n)
            def _(r):
                gather_values(flips, reqbuf[r], sendv, r)
                give_v(r, s).start()

            gather_values(flips, req[s], recvv, s)
            slot_values(s)

    @pl.loop(0, me - 1)
    def _(s):
        give_k(me, s).wait_recv()
        slot_scores(s)

    @pl.loop(0, me - 1)
    def _(s):
        give_sum(me, s).wait_recv()

    @pl.when(me == last)
    def _():
        give_last_sum().wait_recv()

    blocks = n * count
    known = iota((blocks, width), 0) < (me + 1) * count
    sum_k = jnp.where(known, sall[:, 0].reshape(blocks, width).astype(f32), 0.0).astype(bf16)
    sum_v = jnp.where(known, sall[:, 1].reshape(blocks, width).astype(f32), 0.0).astype(bf16)
    flip = flipped(sum_v)
    for g in range(groups):
        svt[g, :DH] = flip[g * DH : (g + 1) * DH]
    part_at = iota((blocks, length), 0)
    time_at = iota((blocks, length), 1) + me * length
    sbias = jnp.where(part_at * CMP_STRIDE + CMP_BLOCK - 1 <= time_at, 0.0, NEG)

    sks[...] = sum_k

    def summary_scores(h):
        return score(sks[:, slab_of(h)], qraw[h])

    def summary_weights(h, raw):
        x = raw + sbias
        peak = jnp.maximum(jnp.max(x, 0, keepdims=True), 0.1 * NEG)
        wsum[h] = jnp.exp2(x - peak).astype(bf16)

    pipelined(heads, 6, summary_scores, summary_weights)

    def summary_values(h):
        return jnp.dot(svt[h // per_group], wsum[h], preferred_element_type=f32)

    def summary_out(h, found):
        stot[h : h + 1] = found[DH : DH + 1]
        sacc[h] = found[:DH]

    pipelined(heads, 4, summary_values, summary_out)

    fetches[8].wait()
    first_gate, second_gate = (1.0 / (1.0 + jnp.exp(-gate_ref[w])) for w in range(2))
    far = jnp.where(me == last, me, jnp.maximum(me - 1, 0))
    peak = lax.fori_loop(0, far, lambda s, x: jnp.maximum(x, slot_top[s]), top[...])
    keep = jnp.exp2(top[...] - peak)
    whole = lax.fori_loop(
        0,
        far,
        lambda s, x: x + slot_total[s] * jnp.exp2(slot_top[s] - peak),
        total[...] * keep,
    )
    shared = second_gate / whole
    keep = keep * shared
    first_gate = first_gate / jnp.maximum(stot[...], 1.0)

    @pl.loop(0, far)
    def _(s):
        slot_top[s] = jnp.exp2(slot_top[s] - peak) * shared

    for h in range(heads):
        acc[h] = sacc[h] * first_gate[h : h + 1] + acc[h] * keep[h : h + 1]

    def finish(pair, heads_mixed):
        both = []
        for mixed in heads_mixed:
            mean = jnp.sum(mixed * mixed, 0, keepdims=True) * (1.0 / DH)
            both.append(mixed * lax.rsqrt(mean + EPS))
        flat = jnp.concatenate(both, 0) * jnp.concatenate([gain_at[pair]] * (length // WIDE), 1)
        out_ref[0, :, pair * WIDE : (pair + 1) * WIDE] = flat.astype(bf16).T

    def heads_of(pair):
        return range(2 * pair, 2 * pair + 2)

    def added(s, h, found):
        return acc[h] + found * slot_top[s, h : h + 1]

    def add_slot(s):
        def second(h, found):
            acc[h] = added(s, h, found)

        pipelined(heads, 4, lambda h: slot_product(s, h), second)

    @pl.when(me == last)
    def _():
        give_last_v().wait_recv()
        add_slot(me - 1)

    @pl.loop(1, me - 1)
    def _(s):
        give_v(me, s).wait_recv()
        add_slot(s)

    @pl.when(me >= 2)
    def _():
        give_v(me, 0).wait_recv()
        pipelined(
            heads // 2,
            4,
            lambda pair: [slot_product(0, h) for h in heads_of(pair)],
            lambda pair, found: finish(
                pair, [added(0, h, x) for h, x in zip(heads_of(pair), found)]
            ),
        )

    @pl.when(me < 2)
    def _():
        for pair in range(heads // 2):
            finish(pair, [acc[h] for h in heads_of(pair)])

    @pl.when(me < last)
    def _():
        give_near(0, me + 1).wait_send()

    @pl.when(me < last - 1)
    def _():
        give_near(1, me + 1).wait_send()

    @pl.when(me == last - 1)
    def _():
        give_last_sum().wait_send()
        give_last_v().wait_send()

    @pl.when(me == last)
    def _():
        give_edge().wait_send()
        ask_last().wait_send()

    @pl.loop(0, me - 1)
    def _(s):
        ask(s, me).wait_send()

    @pl.when(me >= 1)
    def _():
        @pl.loop(me + 1, n)
        def _(r):
            give_k(r, me - 1).wait_send()
            give_v(r, me - 1).wait_send()
            give_sum(r, me - 1).wait_send()


def per_device(queries, keys, values, gate_logits, chosen, pool_k, pool_v, out_gain):
    n = lax.axis_size("kv")
    length = queries.shape[1]
    groups = keys.shape[2] // DH
    heads = queries.shape[2] // DH
    qblocks = length // QB
    per = length // SLC
    count = length // CMP_STRIDE
    lanes = -(-n * per // 128) * 128
    rows = qblocks * groups
    width = groups * DH
    size = MOST * SLC
    slabs = groups // 2
    asked = -(-(MOST * slabs + groups) // 8) * 8
    gates = gate_logits.transpose(0, 1, 3, 2)
    base, shift = rope_constants(n, length)
    bf16, f32, i32 = jnp.bfloat16, jnp.float32, jnp.int32
    vm, dma = pltpu.VMEM, pltpu.SemaphoreType.DMA
    scratch = [
        vm((length, heads * DH), bf16),
        vm((2, length, width), bf16),
        vm((2, heads, length), f32),
        vm(chosen.shape[1:], i32),
        vm((2, CMP_BLOCK, DH), f32),
        vm((1, heads * DH), f32),
        vm(base.shape, f32),
        vm(shift.shape, f32),
        vm((2, length, width), bf16),
        vm((heads, length, WIDE), bf16),
        vm((heads, length, WIDE), bf16),
        vm((length, width), bf16),
        vm((groups, DH + ONES, length), bf16),
        vm((n, 2, count, width), bf16),
        vm((n * count, width), bf16),
        vm((groups, DH + ONES, n * count), bf16),
        vm((heads, n * count, length), bf16),
        vm((MOST * rows, lanes), i32),
        vm((per, rows, QB), f32),
        vm((MOST * rows, QB), f32),
        vm((QB, QB), f32),
        vm((n, asked, WIDE), f32),
        vm((n, asked, WIDE), f32),
        vm((asked, WIDE), f32),
        vm((CMP_STRIDE, width), bf16),
        vm((count, width), bf16),
        vm((n, size, width), bf16),
        vm((n, width, size), bf16),
        vm((n, size, width), bf16),
        vm((n, width, size), bf16),
        vm((n, heads, size, length), bf16),
        vm((n, heads, length), f32),
        vm((n, heads, length), f32),
        vm((heads // 2, WIDE, WIDE), f32),
        vm((heads, length), f32),
        vm((heads, length), f32),
        vm((heads, DH, length), f32),
        vm((heads, length), f32),
        vm((heads, DH, length), f32),
        dma((10,)), dma((2,)), dma((2,)),
        dma((n,)), dma((n,)), dma((n,)), dma((n,)), dma((n,)), dma((n,)), dma((n,)), dma((n,)),
        dma((3,)), dma((3,)),
    ]
    operands = (queries, keys, values, gates, chosen, pool_k, pool_v, out_gain[None], base, shift)
    return pl.pallas_call(
        functools.partial(kernel, n),
        out_shape=jax.ShapeDtypeStruct(queries.shape, bf16),
        in_specs=[pl.BlockSpec(memory_space=pltpu.HBM)] * 10,
        out_specs=pl.BlockSpec(memory_space=pltpu.VMEM),
        scratch_shapes=scratch,
        compiler_params=pltpu.CompilerParams(
            collective_id=0, has_side_effects=True, vmem_limit_bytes=44 << 20
        ),
    )(*(pltpu.with_memory_space_constraint(x, pltpu.HBM) for x in operands))


def solution(mesh):
    in_specs = (
        P(("grp", "dp"), "kv", "tp"),
        P(("grp", "dp"), "kv", "tp"),
        P(("grp", "dp"), "kv", "tp"),
        P(("grp", "dp"), None, "kv", "tp"),
        P(("grp", "dp"), "kv", "tp", None),
        P(),
        P(),
        P("tp"),
    )
    out_specs = P(("grp", "dp"), "kv", "tp")
    return jax.shard_map(
        per_device, mesh=mesh, in_specs=in_specs, out_specs=out_specs, check_vma=False
    )
```

```python
import functools

import jax
import jax.numpy as jnp
import numpy as np
from jax import lax
from jax.experimental import pallas as pl
from jax.experimental.pallas import tpu as pltpu
from jax.sharding import PartitionSpec as P

DH = 64
CMP_STRIDE = 16
CMP_BLOCK = 32
SLC = 64
QB = 128
MOST = 2
THETA = 500000.0
EPS = 1e-06
NEG = -1e30
LOG2E = 1.4426950408889634
WIDE = 2 * DH
ONES = 16
MESH = pl.DeviceIdType.MESH


def rope_constants(n, length):
    half = DH // 2
    freq = THETA ** (-2.0 * (np.arange(WIDE) % half) / DH)
    within = np.arange(length)[:, None] * freq[None, :]
    start = np.arange(n)[:, None] * length * freq[None, :]
    base = np.stack([np.cos(within), np.sin(within)]).astype(np.float32)
    shift = np.stack([np.cos(start), np.sin(start)], 1).astype(np.float32)
    return base, shift


def kernel(
    n, q_hbm, k_hbm, v_hbm, gate_hbm, list_hbm, pk_hbm, pv_hbm, gain_hbm, base_hbm, shift_hbm,
    out_ref,
    q_ref, kv_ref, gate_ref, list_ref, pool_ref, gain_ref, base_ref, shift_ref,
    near, qraw, qt, kt, vt, sall, sks, svt, wsum, flag, own_bias, far_bias, tri,
    req, reqbuf, reqlast, edge, lastsum, sendk, sendv, recvk, recvv, wslot, slot_top, slot_total, gain_at,
    top, total, acc, stot, sacc,
    local, near_send, near_recv, req_send, req_recv, k_send, k_recv, v_send, v_recv,
    sum_send, sum_recv, last_send, last_recv,
):
    me = lax.axis_index("kv")
    length = q_ref.shape[0]
    heads = q_ref.shape[1] // DH
    width = kv_ref.shape[2]
    groups = width // DH
    per_group = heads // groups
    pairs = per_group // 2
    slabs = groups // 2
    qblocks = length // QB
    per = length // SLC
    count = length // CMP_STRIDE
    size = MOST * SLC
    scale = DH ** (-0.5) * LOG2E
    f32, bf16 = jnp.float32, jnp.bfloat16

    barrier = pltpu.get_barrier_semaphore()

    @pl.when(me >= 1)
    def _():
        pl.semaphore_signal(barrier, inc=1, device_id={"kv": me - 1}, device_id_type=MESH)

        @pl.loop(me + 1, n)
        def _(r):
            pl.semaphore_signal(barrier, inc=1, device_id={"kv": r}, device_id_type=MESH)

    fetches = [
        pltpu.make_async_copy(src, dst, local.at[i])
        for i, (src, dst) in enumerate(
            (
                (k_hbm.at[0], kv_ref.at[0]),
                (v_hbm.at[0], kv_ref.at[1]),
                (list_hbm.at[0], list_ref),
                (base_hbm, base_ref),
                (shift_hbm, shift_ref),
                (q_hbm.at[0], q_ref),
                (pk_hbm, pool_ref.at[0]),
                (pv_hbm, pool_ref.at[1]),
                (gate_hbm.at[0], gate_ref),
                (gain_hbm, gain_ref),
            )
        )
    ]
    for fetch in fetches:
        fetch.start()

    def remote(src, dst, send, recv, peer):
        return pltpu.make_async_remote_copy(
            src_ref=src, dst_ref=dst, send_sem=send, recv_sem=recv,
            device_id={"kv": peer}, device_id_type=MESH,
        )

    def give_near(w, peer):
        return remote(kv_ref.at[w], near.at[w], near_send.at[w], near_recv.at[w], peer)

    def ask(s, origin):
        return remote(req.at[s], reqbuf.at[origin], req_send.at[s], req_recv.at[origin], s + 1)

    def give_k(r, s):
        return remote(sendk.at[r], recvk.at[s], k_send.at[r], k_recv.at[s], r)

    def give_v(r, s):
        return remote(sendv.at[r], recvv.at[s], v_send.at[r], v_recv.at[s], r)

    def ask_last():
        return remote(req.at[n - 2], reqlast, last_send.at[0], last_recv.at[0], n - 2)

    def give_edge():
        return remote(
            kv_ref.at[1, pl.ds(0, CMP_STRIDE)], edge, last_send.at[1], last_recv.at[1], n - 2
        )

    def give_last_sum():
        return remote(lastsum, sall.at[n - 2, 1], last_send.at[2], last_recv.at[2], n - 1)

    def give_last_v():
        return remote(sendv.at[0], recvv.at[n - 2], v_send.at[0], v_recv.at[n - 2], n - 1)

    def give_sum(r, s):
        return remote(sall.at[s], sall.at[s], sum_send.at[r], sum_recv.at[s], r)

    def iota(shape, axis):
        return lax.broadcasted_iota(jnp.int32, shape, axis)

    fetches[0].wait()
    fetches[1].wait()
    pl.semaphore_wait(barrier, jnp.where(me < n - 1, 1, 0) + jnp.maximum(me - 1, 0))

    last = n - 1

    @pl.when(me < last)
    def _():
        give_near(0, me + 1).start()

    @pl.when(me < last - 1)
    def _():
        give_near(1, me + 1).start()

    @pl.when(me == last)
    def _():
        give_edge().start()

    lanes = flag.shape[1]
    rows = qblocks * groups

    def column(x, at):
        spot = iota(x.shape, 1) == at
        picked = jnp.sum(jnp.where(spot, x.astype(f32), 0.0), 1, keepdims=True)
        return jnp.broadcast_to(picked, (x.shape[0], QB))

    fetches[2].wait()
    lists = jnp.concatenate([list_ref[b] for b in range(qblocks)], 0)
    lane = iota((rows, lanes), 1)
    member = jnp.zeros((rows, lanes), jnp.int32)
    for i in range(lists.shape[1]):
        member = jnp.where(lists[:, i : i + 1] == lane, 1, member)
    union = member[:groups]
    for b in range(1, qblocks):
        union = jnp.maximum(union, member[b * groups : (b + 1) * groups])
    union = jnp.concatenate([union] * qblocks, 0)
    inner = lane % per
    rank = jnp.zeros_like(union)
    for d in range(1, per):
        rank = rank + jnp.where(inner >= d, pltpu.roll(union, d, 1), 0)

    def first_of(x):
        found = x
        for d in range(1, per):
            found = found + pltpu.roll(x, lanes - d, 1)
        return found

    asked = []
    for j in range(MOST):
        hit = (union == 1) & (rank == j)
        asked.append(first_of(jnp.where(hit, inner, 0))[:groups])
        flag[j * rows : (j + 1) * rows, :] = first_of(jnp.where(hit, member, 0))
    asked = jnp.concatenate(asked, 0)
    low_row = iota((1, WIDE), 1) < DH

    @pl.loop(0, me)
    def _(s):
        ids = column(asked, s * per)
        for j in range(MOST):
            for p in range(slabs):
                at = j * groups + 2 * p
                req[s, j * slabs + p : j * slabs + p + 1, :] = jnp.where(
                    low_row, ids[at : at + 1], ids[at + 1 : at + 2]
                )
        for g in range(groups):
            at = MOST * slabs + g
            req[s, at : at + 1, :] = jnp.where(
                low_row, ids[g : g + 1], ids[groups + g : groups + g + 1]
            )

    @pl.loop(0, me - 1)
    def _(s):
        ask(s, me).start()

    @pl.when(me == last)
    def _():
        ask_last().start()

    for i in range(per):
        own_bias[i] = jnp.where(column(member, me * per + i) > 0.5, 0.0, NEG)
    tri[...] = jnp.where(iota((QB, QB), 0) <= iota((QB, QB), 1), 0.0, NEG)

    def lane_map(shape, source):
        wanted = source(iota((1, shape[1]), 1))
        return jnp.where(iota(shape, 0) == wanted, 1.0, 0.0).astype(bf16)

    half = DH // 2
    partner_map = lane_map((width, width), lambda c: c - c % DH + (c + half) % DH)
    eye = lane_map((width, width), lambda c: c)

    def spread_map(side, turn):
        shape = (per_group * DH, per_group * WIDE)
        return lane_map(
            shape,
            lambda c: jnp.where(
                c % WIDE // DH == side, c // WIDE * DH + (c + turn) % DH, -1
            ),
        )

    def mapped(x, lanes_to):
        return jnp.dot(x, lanes_to, preferred_element_type=f32)

    def score(keys, queries):
        return lax.dot_general(
            keys, queries, (((1,), (1,)), ((), ())), preferred_element_type=f32
        )

    fetches[3].wait()
    fetches[4].wait()
    sign = jnp.where(iota((1, WIDE), 1) % DH < half, -1.0, 1.0)

    def tables(span):
        cos_in, sin_in = base_ref[0], base_ref[1]
        cos_at, sin_at = shift_ref[span, 0:1], shift_ref[span, 1:2]
        cosine = cos_in * cos_at - sin_in * sin_at
        sine = (sin_in * cos_at + cos_in * sin_at) * sign
        return cosine, sine

    def pipelined(steps, ahead, first, second):
        queue = [first(i) for i in range(min(ahead, steps))]
        for i in range(steps):
            if i + ahead < steps:
                queue.append(first(i + ahead))
            second(i, queue.pop(0))

    def turned_slabs(x, cosine, sine):
        other = mapped(x, partner_map)
        found = []
        for p in range(slabs):
            cols = slice(p * WIDE, (p + 1) * WIDE)
            found.append((x[:, cols].astype(f32) * cosine + other[:, cols] * sine).astype(bf16))
        return jnp.concatenate(found, 1)

    cosine, sine = tables(me)
    kt[...] = turned_slabs(kv_ref[0], cosine, sine)

    def flipped(x):
        return score(eye, x).astype(bf16)

    flip = flipped(kv_ref[1])
    for g in range(groups):
        vt[g, :DH] = flip[g * DH : (g + 1) * DH]
        vt[g, DH:] = jnp.ones((ONES, length), bf16)
        svt[g, DH:] = jnp.ones((ONES, n * count), bf16)

    cosine = cosine * scale
    sine = sine * scale
    fetches[5].wait()
    spreads = [(spread_map(side, 0), spread_map(side, half)) for side in range(2)]
    for g in range(groups):
        x = q_ref[:, g * per_group * DH : (g + 1) * per_group * DH]
        plain, other = (mapped(x, lanes_to) for lanes_to in spreads[g % 2])
        for o in range(per_group):
            cols = slice(o * WIDE, (o + 1) * WIDE)
            qraw[g * per_group + o] = plain[:, cols].astype(bf16)
            qt[g * per_group + o] = (plain[:, cols] * cosine + other[:, cols] * sine).astype(bf16)

    def slab_of(h):
        p = h // per_group // 2
        return slice(p * WIDE, (p + 1) * WIDE)

    def own_scores(h):
        return score(kt[:, slab_of(h)], qt[h])

    def own_values(h, raw):
        g = h // per_group
        weights, tops = [], []
        for b in range(qblocks):
            cols = slice(b * QB, (b + 1) * QB)
            parts = []
            for i in range((b + 1) * QB // SLC):
                x = raw[i * SLC : (i + 1) * SLC, cols]
                if i * SLC < b * QB:
                    x = x + own_bias[i, b * groups + g : b * groups + g + 1, :]
                else:
                    x = x + tri[i * SLC - b * QB : (i + 1) * SLC - b * QB, :]
                parts.append(x)
            x = jnp.concatenate(parts, 0)
            peak = jnp.max(x, 0, keepdims=True)
            w = jnp.exp2(x - peak).astype(bf16)
            if x.shape[0] < length:
                w = jnp.concatenate([w, jnp.zeros((length - x.shape[0], QB), bf16)], 0)
            weights.append(w)
            tops.append(peak)
        found = jnp.dot(vt[g], jnp.concatenate(weights, 1), preferred_element_type=f32)
        top[h : h + 1] = jnp.concatenate(tops, 1)
        total[h : h + 1] = found[DH : DH + 1]
        acc[h] = found[:DH]

    pipelined(heads, 6, own_scores, own_values)

    fetches[9].wait()
    for pair in range(heads // 2):
        row = gain_ref[:, pair * WIDE : (pair + 1) * WIDE]
        gain_at[pair] = jnp.broadcast_to(row, (WIDE, WIDE)).T

    fetches[6].wait()
    fetches[7].wait()

    def summarize(w, x, following, p):
        pool = pool_ref[w]
        pool = jnp.concatenate([pool, pool], 1)
        cols = slice(p * WIDE, (p + 1) * WIDE)
        x = x[:, cols].astype(f32)
        after = jnp.concatenate([x[CMP_STRIDE:], following[:, cols].astype(f32)], 0)
        shape = (count, CMP_STRIDE, WIDE)
        z = x.reshape(shape) * pool[None, :CMP_STRIDE] + after.reshape(shape) * pool[None, CMP_STRIDE:]
        found = jnp.sum(z, 1)
        return (found * scale if w == 0 else found).astype(bf16)

    for w in range(2):
        for p in range(slabs):
            sall[me, w, :, p * WIDE : (p + 1) * WIDE] = summarize(
                w, kv_ref[w], jnp.zeros((CMP_STRIDE, width), bf16), p
            )

    def gather(source, w_rows, dst, at):
        for j in range(MOST):
            for p in range(slabs):
                cols = slice(p * WIDE, (p + 1) * WIDE)
                pick = w_rows[j * slabs + p : j * slabs + p + 1, :]
                block = None
                for i in range(per):
                    weight = jnp.broadcast_to(jnp.where(pick == i, 1.0, 0.0), (SLC, WIDE))
                    term = source[i * SLC : (i + 1) * SLC, cols] * weight.astype(bf16)
                    block = term if block is None else block + term
                dst[at, j * SLC : (j + 1) * SLC, cols] = block

    def turned_values(x):
        swapped = [x[(i ^ 1) * SLC : ((i ^ 1) + 1) * SLC] for i in range(per)]
        return score(eye, jnp.concatenate([x, *swapped], 0)).astype(bf16)

    side_row = jnp.where(low_row, 0.0, 1.0)

    def gather_values(flips, w_rows, dst, at):
        for g in range(groups):
            span = slice(g * DH, (g + 1) * DH)
            pick = w_rows[MOST * slabs + g : MOST * slabs + g + 1, :]
            block = None
            for swap in range(2):
                for c in range(per // 2):
                    wanted = jnp.abs(side_row - swap) + 2 * c
                    weight = jnp.broadcast_to(jnp.where(pick == wanted, 1.0, 0.0), (DH, WIDE))
                    start = swap * length + c * WIDE
                    term = flips[span, start : start + WIDE] * weight.astype(bf16)
                    block = term if block is None else block + term
            dst[at, span, :] = block

    def slot_scores(s):
        far_bias[...] = jnp.where(column(flag[...], s * per) > 0.5, 0.0, NEG)

        def first(h):
            return score(recvk[s, :, slab_of(h)], qt[h])

        def second(h, raw):
            g = h // per_group
            rowed = [
                jnp.concatenate(
                    [far_bias[(j * qblocks + b) * groups + g][None] for b in range(qblocks)], 1
                )
                for j in range(MOST)
            ]
            cut = [raw[j * SLC : (j + 1) * SLC] for j in range(MOST)]
            peak = functools.reduce(
                jnp.maximum,
                [jnp.max(x, 0, keepdims=True) + row for x, row in zip(cut, rowed)],
            )
            peak = jnp.maximum(peak, 0.1 * NEG)
            slot_top[s, h : h + 1] = peak
            sums = []
            for j in range(MOST):
                w = jnp.exp2(cut[j] - (peak - rowed[j]))
                sums.append(jnp.sum(w, 0, keepdims=True))
                wslot[s, h, j * SLC : (j + 1) * SLC] = w.astype(bf16)
            slot_total[s, h : h + 1] = functools.reduce(jnp.add, sums)

        pipelined(heads, 6, first, second)

    def slot_product(s, h):
        g = h // per_group
        return jnp.dot(
            recvv[s, g * DH : (g + 1) * DH, :], wslot[s, h], preferred_element_type=f32
        )

    def slot_values(s):
        old, fresh = top[...], slot_top[s]
        peak = jnp.maximum(old, fresh)
        keep, gain = jnp.exp2(old - peak), jnp.exp2(fresh - peak)
        top[...] = peak
        total[...] = total[...] * keep + slot_total[s] * gain

        def second(h, found):
            acc[h] = acc[h] * keep[h : h + 1] + found * gain[h : h + 1]

        pipelined(heads, 8, lambda h: slot_product(s, h), second)

    @pl.when(me == last - 1)
    def _():
        flips = turned_values(kv_ref[1])
        give_edge().wait_recv()
        for p in range(slabs):
            lastsum[:, p * WIDE : (p + 1) * WIDE] = summarize(1, kv_ref[1], edge[...], p)
        ask_last().wait_recv()
        gather_values(flips, reqlast, sendv, 0)
        give_last_sum().start()
        give_last_v().start()

    @pl.when(me >= 1)
    def _():
        s = me - 1
        give_near(0, me).wait_recv()
        turned = turned_slabs(near[0], *tables(s))

        @pl.loop(0, last - me)
        def _(d):
            r = last - d
            ask(s, r).wait_recv()
            gather(turned, reqbuf[r], sendk, r)
            give_k(r, s).start()

        gather(turned, req[s], recvk, s)
        for p in range(slabs):
            sall[s, 0, :, p * WIDE : (p + 1) * WIDE] = summarize(
                0, near[0], kv_ref[0, :CMP_STRIDE], p
            )
        slot_scores(s)

        @pl.when(me < last)
        def _():
            give_near(1, me).wait_recv()
            for p in range(slabs):
                sall[s, 1, :, p * WIDE : (p + 1) * WIDE] = summarize(
                    1, near[1], kv_ref[1, :CMP_STRIDE], p
                )

            @pl.loop(me + 1, n)
            def _(r):
                give_sum(r, s).start()

            flips = turned_values(near[1])

            @pl.loop(me + 1, n)
            def _(r):
                gather_values(flips, reqbuf[r], sendv, r)
                give_v(r, s).start()

            gather_values(flips, req[s], recvv, s)
            slot_values(s)

    @pl.loop(0, me - 1)
    def _(s):
        give_k(me, s).wait_recv()
        slot_scores(s)

    @pl.loop(0, me - 1)
    def _(s):
        give_sum(me, s).wait_recv()

    @pl.when(me == last)
    def _():
        give_last_sum().wait_recv()

    blocks = n * count
    known = iota((blocks, width), 0) < (me + 1) * count
    sum_k = jnp.where(known, sall[:, 0].reshape(blocks, width).astype(f32), 0.0).astype(bf16)
    sum_v = jnp.where(known, sall[:, 1].reshape(blocks, width).astype(f32), 0.0).astype(bf16)
    flip = flipped(sum_v)
    for g in range(groups):
        svt[g, :DH] = flip[g * DH : (g + 1) * DH]
    part_at = iota((blocks, length), 0)
    time_at = iota((blocks, length), 1) + me * length
    sbias = jnp.where(part_at * CMP_STRIDE + CMP_BLOCK - 1 <= time_at, 0.0, NEG)

    sks[...] = sum_k

    def summary_scores(h):
        return score(sks[:, slab_of(h)], qraw[h])

    def summary_weights(h, raw):
        x = raw + sbias
        peak = jnp.maximum(jnp.max(x, 0, keepdims=True), 0.1 * NEG)
        wsum[h] = jnp.exp2(x - peak).astype(bf16)

    pipelined(heads, 10, summary_scores, summary_weights)

    def summary_values(h):
        return jnp.dot(svt[h // per_group], wsum[h], preferred_element_type=f32)

    def summary_out(h, found):
        stot[h : h + 1] = found[DH : DH + 1]
        sacc[h] = found[:DH]

    pipelined(heads, 8, summary_values, summary_out)

    fetches[8].wait()
    first_gate, second_gate = (1.0 / (1.0 + jnp.exp(-gate_ref[w])) for w in range(2))
    far = jnp.where(me == last, me, jnp.maximum(me - 1, 0))
    peak = lax.fori_loop(0, far, lambda s, x: jnp.maximum(x, slot_top[s]), top[...])
    keep = jnp.exp2(top[...] - peak)
    whole = lax.fori_loop(
        0,
        far,
        lambda s, x: x + slot_total[s] * jnp.exp2(slot_top[s] - peak),
        total[...] * keep,
    )
    shared = second_gate / whole
    keep = keep * shared
    first_gate = first_gate / jnp.maximum(stot[...], 1.0)

    @pl.loop(0, far)
    def _(s):
        slot_top[s] = jnp.exp2(slot_top[s] - peak) * shared

    for h in range(heads):
        acc[h] = sacc[h] * first_gate[h : h + 1] + acc[h] * keep[h : h + 1]

    def finish(pair, heads_mixed):
        both = []
        for mixed in heads_mixed:
            mean = jnp.sum(mixed * mixed, 0, keepdims=True) * (1.0 / DH)
            both.append(mixed * lax.rsqrt(mean + EPS))
        flat = jnp.concatenate(both, 0) * jnp.concatenate([gain_at[pair]] * (length // WIDE), 1)
        out_ref[0, :, pair * WIDE : (pair + 1) * WIDE] = flat.astype(bf16).T

    def heads_of(pair):
        return range(2 * pair, 2 * pair + 2)

    def added(s, h, found):
        return acc[h] + found * slot_top[s, h : h + 1]

    def add_slot(s):
        def second(h, found):
            acc[h] = added(s, h, found)

        pipelined(heads, 8, lambda h: slot_product(s, h), second)

    @pl.when(me == last)
    def _():
        give_last_v().wait_recv()
        add_slot(me - 1)

    @pl.loop(1, me - 1)
    def _(s):
        give_v(me, s).wait_recv()
        add_slot(s)

    @pl.when(me >= 2)
    def _():
        give_v(me, 0).wait_recv()
        pipelined(
            heads // 2,
            4,
            lambda pair: [slot_product(0, h) for h in heads_of(pair)],
            lambda pair, found: finish(
                pair, [added(0, h, x) for h, x in zip(heads_of(pair), found)]
            ),
        )

    @pl.when(me < 2)
    def _():
        for pair in range(heads // 2):
            finish(pair, [acc[h] for h in heads_of(pair)])

    @pl.when(me < last)
    def _():
        give_near(0, me + 1).wait_send()

    @pl.when(me < last - 1)
    def _():
        give_near(1, me + 1).wait_send()

    @pl.when(me == last - 1)
    def _():
        give_last_sum().wait_send()
        give_last_v().wait_send()

    @pl.when(me == last)
    def _():
        give_edge().wait_send()
        ask_last().wait_send()

    @pl.loop(0, me - 1)
    def _(s):
        ask(s, me).wait_send()

    @pl.when(me >= 1)
    def _():
        @pl.loop(me + 1, n)
        def _(r):
            give_k(r, me - 1).wait_send()
            give_v(r, me - 1).wait_send()
            give_sum(r, me - 1).wait_send()


def per_device(queries, keys, values, gate_logits, chosen, pool_k, pool_v, out_gain):
    n = lax.axis_size("kv")
    length = queries.shape[1]
    groups = keys.shape[2] // DH
    heads = queries.shape[2] // DH
    qblocks = length // QB
    per = length // SLC
    count = length // CMP_STRIDE
    lanes = -(-n * per // 128) * 128
    rows = qblocks * groups
    width = groups * DH
    size = MOST * SLC
    slabs = groups // 2
    asked = -(-(MOST * slabs + groups) // 8) * 8
    gates = gate_logits.transpose(0, 1, 3, 2)
    base, shift = rope_constants(n, length)
    bf16, f32, i32 = jnp.bfloat16, jnp.float32, jnp.int32
    vm, dma = pltpu.VMEM, pltpu.SemaphoreType.DMA
    scratch = [
        vm((length, heads * DH), bf16),
        vm((2, length, width), bf16),
        vm((2, heads, length), f32),
        vm(chosen.shape[1:], i32),
        vm((2, CMP_BLOCK, DH), f32),
        vm((1, heads * DH), f32),
        vm(base.shape, f32),
        vm(shift.shape, f32),
        vm((2, length, width), bf16),
        vm((heads, length, WIDE), bf16),
        vm((heads, length, WIDE), bf16),
        vm((length, width), bf16),
        vm((groups, DH + ONES, length), bf16),
        vm((n, 2, count, width), bf16),
        vm((n * count, width), bf16),
        vm((groups, DH + ONES, n * count), bf16),
        vm((heads, n * count, length), bf16),
        vm((MOST * rows, lanes), i32),
        vm((per, rows, QB), f32),
        vm((MOST * rows, QB), f32),
        vm((QB, QB), f32),
        vm((n, asked, WIDE), f32),
        vm((n, asked, WIDE), f32),
        vm((asked, WIDE), f32),
        vm((CMP_STRIDE, width), bf16),
        vm((count, width), bf16),
        vm((n, size, width), bf16),
        vm((n, width, size), bf16),
        vm((n, size, width), bf16),
        vm((n, width, size), bf16),
        vm((n, heads, size, length), bf16),
        vm((n, heads, length), f32),
        vm((n, heads, length), f32),
        vm((heads // 2, WIDE, WIDE), f32),
        vm((heads, length), f32),
        vm((heads, length), f32),
        vm((heads, DH, length), f32),
        vm((heads, length), f32),
        vm((heads, DH, length), f32),
        dma((10,)), dma((2,)), dma((2,)),
        dma((n,)), dma((n,)), dma((n,)), dma((n,)), dma((n,)), dma((n,)), dma((n,)), dma((n,)),
        dma((3,)), dma((3,)),
    ]
    operands = (queries, keys, values, gates, chosen, pool_k, pool_v, out_gain[None], base, shift)
    return pl.pallas_call(
        functools.partial(kernel, n),
        out_shape=jax.ShapeDtypeStruct(queries.shape, bf16),
        in_specs=[pl.BlockSpec(memory_space=pltpu.HBM)] * 10,
        out_specs=pl.BlockSpec(memory_space=pltpu.VMEM),
        scratch_shapes=scratch,
        compiler_params=pltpu.CompilerParams(
            collective_id=0, has_side_effects=True, vmem_limit_bytes=44 << 20
        ),
    )(*(pltpu.with_memory_space_constraint(x, pltpu.HBM) for x in operands))


def solution(mesh):
    in_specs = (
        P(("grp", "dp"), "kv", "tp"),
        P(("grp", "dp"), "kv", "tp"),
        P(("grp", "dp"), "kv", "tp"),
        P(("grp", "dp"), None, "kv", "tp"),
        P(("grp", "dp"), "kv", "tp", None),
        P(),
        P(),
        P("tp"),
    )
    out_specs = P(("grp", "dp"), "kv", "tp")
    return jax.shard_map(
        per_device, mesh=mesh, in_specs=in_specs, out_specs=out_specs, check_vma=False
    )
```
